768 devices in a mesh: rep: 3 (over z_hi), fs: 32 (over z_lo, y), tp: 8 (over x, core).
Axes of the slice: x: 4, y: 8, z: 12 (z_hi: 3, z_lo: 4; z = z_hi * 4 + z_lo), core: 2. Of those that a mesh axis runs over, the one named last changes fastest.
Arguments:
- out_grad: bfloat16 [24576, 2048], P(('rep', 'fs'), 'tp'), may hold values from -6 to 6
- gate_lin: bfloat16 [24576, 5632], P(('rep', 'fs'), 'tp'), may hold values from -6 to 6
- up_lin: bfloat16 [24576, 5632], P(('rep', 'fs'), 'tp'), may hold values from -6 to 6
- conv_weight: bfloat16 [3, 5632], replicated, may hold values from -3.5 to 3.5
- gate_weight: bfloat16 [2048, 5632], P('fs', 'tp'), may hold values from -0.125 to 0.125
- up_weight: bfloat16 [2048, 5632], P('fs', 'tp'), may hold values from -0.125 to 0.125
- down_weight: bfloat16 [5632, 2048], P('tp', 'fs'), may hold values from -0.078125 to 0.078125
Outputs:
- input_grad: bfloat16 [24576, 2048], P(('rep', 'fs'), 'tp')
- conv_grad: float32 [3, 5632], replicated
The draws below stay inside these ranges and needn't reach their ends.
All inputs are finite; a program needn't handle non-finite values.
Results may differ from the reference program's by a relative error of at most 0.015.
Values may be sent and summed in bfloat16 or wider, within the bound.
No kernel may reach another device: no remote copies, remote signals or barrier semaphores. Data moves between devices by JAX's collectives and lax.ppermute only.
A program may use at most 64 MiB of HBM per device.

```python
import math
from functools import partial
import jax
import jax.numpy as jnp
from jax import lax

D = 2048
FF = 5632
SEQ = 8192
SEQS = 3
TOKENS = 24576
N_TP = 8


def shard_levels(key, shape, pieces, low, top_value):
    level, own = 1.0, jax.random.fold_in(key, 6)
    for axis_at, parts in pieces:
        heights = jnp.exp(jax.random.uniform(jax.random.fold_in(own, axis_at), (parts,), jnp.float32, low / len(pieces), top_value / len(pieces)))
        level = level * jnp.repeat(heights, shape[axis_at] // parts).reshape([-1 if axis == axis_at else 1 for axis in range(len(shape))])
    return level


def normal_values(stream_key, shape, spread, bound, split=(), held_as=jnp.bfloat16):
    gain = shard_levels(stream_key, shape, split, -0.22, 0.18) if split else 1.0
    drawn = jax.random.normal(stream_key, shape, jnp.float32) * spread * gain
    return jnp.minimum(jnp.maximum(drawn, -bound), bound).astype(held_as)


def setup_inputs(seed: int = 0) -> dict:
    streams_of = jax.random.split(jax.random.key(seed), 8)
    out_grad = normal_values(streams_of[0], (TOKENS, D), 1.0, 6.0, ((0, 96), (1, 8)))
    gate_lin = normal_values(streams_of[1], (TOKENS, FF), 1.0, 6.0, ((0, 96), (1, 8)))
    up_lin = normal_values(streams_of[2], (TOKENS, FF), 1.0, 6.0, ((0, 96), (1, 8)))
    conv_weight = normal_values(streams_of[3], (3, FF), 3 ** -0.5, 3.5)
    gate_weight = normal_values(streams_of[4], (D, FF), D ** -0.5, 0.125, ((0, 32), (1, 8)))
    up_weight = normal_values(streams_of[5], (D, FF), D ** -0.5, 0.125, ((0, 32), (1, 8)))
    down_weight = normal_values(streams_of[6], (FF, D), FF ** -0.5, 0.078125, ((0, 8), (1, 32)))
    return dict(out_grad=out_grad, gate_lin=gate_lin, up_lin=up_lin, conv_weight=conv_weight, gate_weight=gate_weight, up_weight=up_weight, down_weight=down_weight)


def gelu_parts(gate):
    normal_cdf = 0.5 * (1.0 + jax.scipy.special.erf(gate * (1.0 / math.sqrt(2.0))))
    density = jnp.exp(-0.5 * gate * gate) * (1.0 / math.sqrt(2.0 * math.pi))
    return (gate * normal_cdf, normal_cdf + gate * density)

def shifted(values):
    zero_row = jnp.zeros_like(values[:1])
    before = jnp.concatenate([zero_row, values[:-1]], axis=0)
    after = jnp.concatenate([values[1:], zero_row], axis=0)
    return (before, after)

def one_sequence(packed, conv_weight, gate_weight, up_weight, down_weight):
    grad_block, gate_block, up_block = packed
    conv_taps = conv_weight.astype(jnp.float32)
    linear = gate_block.astype(jnp.float32)
    before, after = shifted(linear)
    gate = conv_taps[0] * before + conv_taps[1] * linear + conv_taps[2] * after
    gelu_value, gelu_slope = gelu_parts(gate)
    act_grad = jnp.dot(grad_block, down_weight.T, preferred_element_type=jnp.float32)
    gate_grad = act_grad * up_block.astype(jnp.float32) * gelu_slope
    up_grad = (act_grad * gelu_value).astype(jnp.bfloat16)
    grad_before, grad_after = shifted(gate_grad)
    linear_grad = (conv_taps[0] * grad_after + conv_taps[1] * gate_grad + conv_taps[2] * grad_before).astype(jnp.bfloat16)
    conv_grad = jnp.stack([lax.optimization_barrier(jnp.sum(gate_grad * before, axis=0)), lax.optimization_barrier(jnp.sum(gate_grad * linear, axis=0)), lax.optimization_barrier(jnp.sum(gate_grad * after, axis=0))])
    block_width = FF // N_TP
    summed = jnp.zeros((grad_block.shape[0], D), jnp.float32)
    for block_index in range(N_TP):
        column_low = block_index * block_width
        column_high = column_low + block_width
        partial_sum = jnp.dot(linear_grad[:, column_low:column_high], gate_weight[:, column_low:column_high].T, preferred_element_type=jnp.float32)
        partial_sum = partial_sum + jnp.dot(up_grad[:, column_low:column_high], up_weight[:, column_low:column_high].T, preferred_element_type=jnp.float32)
        rounded = lax.optimization_barrier(partial_sum.astype(jnp.bfloat16))
        summed = summed + rounded.astype(jnp.float32)
    return (summed.astype(jnp.bfloat16), conv_grad)

def reference(out_grad, gate_lin, up_lin, conv_weight, gate_weight, up_weight, down_weight):
    grads = out_grad.reshape(SEQS, SEQ, D)
    gates = gate_lin.reshape(SEQS, SEQ, FF)
    ups = up_lin.reshape(SEQS, SEQ, FF)
    worker = partial(one_sequence, conv_weight=conv_weight, gate_weight=gate_weight, up_weight=up_weight, down_weight=down_weight)
    input_blocks, conv_parts = lax.map(worker, (grads, gates, ups))
    return (input_blocks.reshape(TOKENS, D), lax.optimization_barrier(jnp.sum(conv_parts, axis=0)))
```

```python
import math

import jax
import jax.numpy as jnp
from jax import lax
from jax.sharding import Mesh
from jax.sharding import PartitionSpec as P


Z_ALL = ("rep", "z")
SEQ_AXES = ("z", "y")
TP = ("x", "core")
ROWS = ("rep", "z", "y")


def shifted(value, axis, by):
    count = lax.axis_size(axis)
    return lax.ppermute(value, axis, [(i, (i + by) % count) for i in range(count)])


def to_next(value, axis, by):
    count = lax.axis_size(axis)
    pairs = [(i, i + by) for i in range(count) if 0 <= i + by < count]
    return lax.ppermute(value, axis, pairs)


def sent_to_all(value, axis):
    peers = lax.axis_size(axis)
    return lax.all_to_all(
        jnp.broadcast_to(value[None], (peers, *value.shape)), axis, 0, 0, tiled=True
    )


def gathered_z(block):
    count = lax.axis_size("z")
    relative = jnp.stack(
        [block, shifted(block, Z_ALL, -1), shifted(block, Z_ALL, 2), shifted(block, Z_ALL, 1)]
    )
    start = (count - lax.axis_index("z")) % count
    twice = jnp.concatenate([relative, relative])
    ordered = lax.dynamic_slice_in_dim(twice, start, count, 0)
    return ordered.reshape(-1, block.shape[1])


def gathered_y(block):
    half = block.shape[0] // 2
    pieces = {0: block}
    up = down = block
    for k in range(1, 4):
        up = shifted(up, "y", 1)
        down = shifted(down, "y", -1)
        pieces[-k] = up
        pieces[k] = down
    pieces[4] = jnp.concatenate([shifted(up[:half], "y", 1), shifted(down[half:], "y", -1)])
    return pieces


def gelu_parts(gate):
    normal_cdf = 0.5 * (1.0 + jax.scipy.special.erf(gate * (1.0 / math.sqrt(2.0))))
    density = jnp.exp(-0.5 * gate * gate) * (1.0 / math.sqrt(2.0 * math.pi))
    return (gate * normal_cdf, normal_cdf + gate * density)


def local(out_grad, gate_lin, up_lin, conv_weight, gate_weight, up_weight, down_weight):
    rows, columns = gate_lin.shape
    width = out_grad.shape[1]
    z_count, y_count = lax.axis_size("z"), lax.axis_size("y")
    share = gate_weight.shape[0]
    per_tp = width // share
    halves = y_count // per_tp
    y_at = lax.axis_index("y")
    taps = lax.dynamic_slice_in_dim(
        conv_weight, lax.axis_index(TP) * columns, columns, 1
    ).astype(jnp.float32)

    down_pieces = gathered_y(gathered_z(down_weight.T))
    both_pieces = gathered_y(
        gathered_z(jnp.concatenate([gate_weight, up_weight]))
    )

    grads = sent_to_all(out_grad, TP)
    grads = grads.reshape(z_count, halves, rows, per_tp, share)
    grads = grads.transpose(1, 3, 2, 0, 4).reshape(y_count, rows, z_count * share)

    before = to_next(gate_lin[-1:], SEQ_AXES, 1).astype(jnp.float32)
    after = to_next(gate_lin[:1], SEQ_AXES, -1).astype(jnp.float32)
    linear = gate_lin.astype(jnp.float32)
    prev_linear = jnp.concatenate([before, linear[:-1]])
    next_linear = jnp.concatenate([linear[1:], after])
    gate = taps[0] * prev_linear + taps[1] * linear + taps[2] * next_linear
    gelu_value, gelu_slope = gelu_parts(gate)

    act_grad = jnp.zeros((rows, columns), jnp.float32)
    for k, piece in down_pieces.items():
        part = lax.dynamic_index_in_dim(grads, (y_at + k) % y_count, 0, keepdims=False)
        act_grad = act_grad + jnp.dot(part, piece, preferred_element_type=jnp.float32)

    gate_grad = act_grad * up_lin.astype(jnp.float32) * gelu_slope
    up_grad = (act_grad * gelu_value).astype(jnp.bfloat16)
    grad_before = to_next(gate_grad[-1:], SEQ_AXES, 1)
    grad_after = to_next(gate_grad[:1], SEQ_AXES, -1)
    prev_grad = jnp.concatenate([grad_before, gate_grad[:-1]])
    next_grad = jnp.concatenate([gate_grad[1:], grad_after])
    linear_grad = (taps[0] * next_grad + taps[1] * gate_grad + taps[2] * prev_grad).astype(
        jnp.bfloat16
    )

    conv = jnp.stack(
        [
            jnp.sum(gate_grad * prev_linear, axis=0),
            jnp.sum(gate_grad * linear, axis=0),
            jnp.sum(gate_grad * next_linear, axis=0),
        ]
    )
    conv = sent_to_all(conv, Z_ALL).sum(axis=0)
    conv = sent_to_all(conv, "y").sum(axis=0)
    conv = sent_to_all(conv, TP)
    conv_grad = conv.transpose(1, 0, 2).reshape(3, -1)

    contract = (((1,), (1,)), ((), ()))
    product = jnp.zeros((y_count, rows, z_count * share), jnp.bfloat16)
    for k, piece in both_pieces.items():
        piece = piece.reshape(z_count, 2, share, columns)
        gate_piece = piece[:, 0].reshape(-1, columns)
        up_piece = piece[:, 1].reshape(-1, columns)
        part = lax.dot_general(
            linear_grad, gate_piece, contract, preferred_element_type=jnp.float32
        ) + lax.dot_general(up_grad, up_piece, contract, preferred_element_type=jnp.float32)
        product = lax.dynamic_update_index_in_dim(
            product, part.astype(jnp.bfloat16), (y_at + k) % y_count, 0
        )
    product = product.reshape(halves, per_tp, rows, z_count, share)
    product = product.transpose(3, 0, 2, 1, 4).reshape(-1, rows, width)
    arrived = lax.all_to_all(product, TP, 0, 0, tiled=True)
    input_grad = arrived.astype(jnp.float32).sum(axis=0).astype(jnp.bfloat16)
    return (input_grad, conv_grad)


def solution(mesh):
    finer = Mesh(
        mesh.devices.reshape(mesh.shape["rep"], 4, 8, 4, 2), ("rep", "z", "y", "x", "core")
    )
    return jax.shard_map(
        local,
        mesh=finer,
        in_specs=(
            P(ROWS, TP),
            P(ROWS, TP),
            P(ROWS, TP),
            P(),
            P(SEQ_AXES, TP),
            P(SEQ_AXES, TP),
            P(TP, SEQ_AXES),
        ),
        out_specs=(P(ROWS, TP), P()),
        check_vma=False,
    )
```

```python
import math

import jax
import jax.numpy as jnp
from jax import lax
from jax.sharding import Mesh
from jax.sharding import PartitionSpec as P


Z_ALL = ("rep", "zk", "zp")
SEQ_AXES = ("zk", "zp", "y")
TP = ("x", "core")
GROUP = ("zp", "x", "core")
ROWS = ("rep", "zk", "zp", "y")
PAD = 264


def shifted(value, axis, by):
    count = lax.axis_size(axis)
    return lax.ppermute(value, axis, [(i, (i + by) % count) for i in range(count)])


def to_next(value, axis, by):
    count = lax.axis_size(axis)
    pairs = [(i, i + by) for i in range(count) if 0 <= i + by < count]
    return lax.ppermute(value, axis, pairs)


def sent_to_all(value, axis):
    peers = lax.axis_size(axis)
    return lax.all_to_all(
        jnp.broadcast_to(value[None], (peers, *value.shape)), axis, 0, 0, tiled=True
    )


def halves_of(value, second):
    half = value.shape[-1] // 2
    left, right = value[..., :half], value[..., half:]
    return jnp.where(second, right, left), jnp.where(second, left, right)


def gathered_z(own, other):
    relative = [
        own, shifted(other, Z_ALL, -1), shifted(own, Z_ALL, 2), shifted(other, Z_ALL, 1)
    ]
    count = len(relative)
    at = lax.axis_index(("zk", "zp"))
    return jnp.stack(
        [lax.select_n((place - at) % count, *relative) for place in range(count)], axis=1
    )


def gathered_y(block):
    pieces = [(0, 0, block)]
    half = block.shape[1] // 2
    up = down = block
    for k in range(1, 4):
        up = shifted(up, "y", 1)
        down = shifted(down, "y", -1)
        pieces += [(-k, 0, up), (k, 0, down)]
    pieces.append((4, 0, shifted(up[:, :half], "y", 1)))
    pieces.append((4, half, shifted(down[:, half:], "y", -1)))
    count, y_at = lax.axis_size("y"), lax.axis_index("y")
    parts, z_count, share, columns = block.shape
    whole = jnp.zeros((parts, z_count, count, share, columns), block.dtype)
    for k, first, piece in pieces:
        whole = lax.dynamic_update_slice(
            whole, piece[:, :, None], (0, first, (y_at + k) % count, 0, 0)
        )
    return whole.reshape(parts, -1, columns)


def gelu_parts(gate):
    normal_cdf = 0.5 * (1.0 + jax.scipy.special.erf(gate * (1.0 / math.sqrt(2.0))))
    density = jnp.exp(-0.5 * gate * gate) * (1.0 / math.sqrt(2.0 * math.pi))
    return (gate * normal_cdf, normal_cdf + gate * density)


def local(out_grad, gate_lin, up_lin, conv_weight, gate_weight, up_weight, down_weight):
    rows, columns = gate_lin.shape
    width = out_grad.shape[1]
    half = columns // 2
    second = lax.axis_index("zp") == 1

    own, other = halves_of(jnp.stack([down_weight.T, gate_weight, up_weight]), second)
    down_full, gate_full, up_full = gathered_y(gathered_z(own, other))

    spare = ((0, 0), (0, columns - width))
    before = to_next(
        jnp.concatenate([gate_lin[-2:], up_lin[-1:], jnp.pad(out_grad[-1:], spare)]), SEQ_AXES, 1
    )
    after = to_next(
        jnp.concatenate([gate_lin[:2], up_lin[:1], jnp.pad(out_grad[:1], spare)]), SEQ_AXES, -1
    )
    grads = jnp.concatenate(
        [
            before[3:, :width],
            out_grad,
            after[3:, :width],
            jnp.zeros((PAD - rows - 2, width), out_grad.dtype),
        ]
    )
    grads = sent_to_all(grads, GROUP).reshape(2, -1, PAD, width)
    grads = grads.transpose(0, 2, 1, 3).reshape(2 * PAD, -1)

    saved = jnp.concatenate(
        [before[:2], gate_lin, after[:2], before[2:3], up_lin, after[2:3]]
    )
    kept, sent = halves_of(saved, second)
    came = lax.ppermute(sent, "zp", [(0, 1), (1, 0)])
    pair = jnp.stack([jnp.where(second, came, kept), jnp.where(second, kept, came)])
    pair = pair.astype(jnp.float32)
    linear, up_ext = pair[:, : rows + 4], pair[:, rows + 4 :]
    start = lax.axis_index(TP) * columns + jnp.where(second, half, 0)
    taps = lax.dynamic_slice_in_dim(conv_weight, start, half, 1).astype(jnp.float32)

    gate = taps[0] * linear[:, :-2] + taps[1] * linear[:, 1:-1] + taps[2] * linear[:, 2:]
    gelu_value, gelu_slope = gelu_parts(gate)

    act_grad = jnp.dot(grads, down_full, preferred_element_type=jnp.float32)
    act_grad = act_grad.reshape(2, PAD, half)[:, : rows + 2]
    gate_grad = act_grad * up_ext * gelu_slope
    up_grad = (act_grad * gelu_value)[:, 1:-1].astype(jnp.bfloat16)
    own_grad = gate_grad[:, 1:-1]
    linear_grad = (
        taps[0] * gate_grad[:, 2:] + taps[1] * own_grad + taps[2] * gate_grad[:, :-2]
    ).astype(jnp.bfloat16)

    conv = jnp.stack(
        [jnp.sum(own_grad * linear[:, 1 + k : 1 + k + rows], axis=(0, 1)) for k in range(3)]
    )
    conv = sent_to_all(conv, Z_ALL)
    conv = conv.reshape(-1, 2, 3, half).sum(axis=0).transpose(1, 0, 2).reshape(3, columns)
    conv = sent_to_all(conv, "y").sum(axis=0)
    conv = sent_to_all(conv, TP)
    conv_grad = conv.transpose(1, 0, 2).reshape(3, -1)

    contract = (((1,), (1,)), ((), ()))
    product = lax.dot_general(
        linear_grad.reshape(-1, half), gate_full, contract, preferred_element_type=jnp.float32
    ) + lax.dot_general(
        up_grad.reshape(-1, half), up_full, contract, preferred_element_type=jnp.float32
    )
    product = product.astype(jnp.bfloat16).reshape(2, rows, -1, width)
    product = product.transpose(0, 2, 1, 3).reshape(-1, rows, width)
    arrived = lax.all_to_all(product, GROUP, 0, 0, tiled=True)
    input_grad = arrived.astype(jnp.float32).sum(axis=0).astype(jnp.bfloat16)
    return (input_grad, conv_grad)


def solution(mesh):
    finer = Mesh(
        mesh.devices.reshape(mesh.shape["rep"], 2, 2, 8, 4, 2),
        ("rep", "zk", "zp", "y", "x", "core"),
    )
    return jax.shard_map(
        local,
        mesh=finer,
        in_specs=(
            P(ROWS, TP),
            P(ROWS, TP),
            P(ROWS, TP),
            P(),
            P(SEQ_AXES, TP),
            P(SEQ_AXES, TP),
            P(TP, SEQ_AXES),
        ),
        out_specs=(P(ROWS, TP), P()),
        check_vma=False,
    )
```

```python
import math

import jax
import jax.numpy as jnp
from jax import lax
from jax.sharding import Mesh
from jax.sharding import PartitionSpec as P


Z_ALL = ("rep", "zk", "zp")
SEQ_AXES = ("zk", "zp", "y")
TP = ("x", "core")
GROUP = ("zp", "x", "core")
ROWS = ("rep", "zk", "zp", "y")
PAD = 264


def shifted(value, axis, by):
    count = lax.axis_size(axis)
    return lax.ppermute(value, axis, [(i, (i + by) % count) for i in range(count)])


def to_next(value, axis, by):
    count = lax.axis_size(axis)
    pairs = [(i, i + by) for i in range(count) if 0 <= i + by < count]
    return lax.ppermute(value, axis, pairs)


def swapped(value, axis, bit):
    return lax.ppermute(value, axis, [(i, i ^ bit) for i in range(lax.axis_size(axis))])


def sent_to_all(value, axis):
    peers = lax.axis_size(axis)
    return lax.all_to_all(
        jnp.broadcast_to(value[None], (peers, *value.shape)), axis, 0, 0, tiled=True
    )


def halves_of(value, second):
    half = value.shape[-1] // 2
    left, right = value[..., :half], value[..., half:]
    return jnp.where(second, right, left), jnp.where(second, left, right)


def gathered_z(own, other):
    relative = [
        own, shifted(other, Z_ALL, -1), shifted(own, Z_ALL, 2), shifted(other, Z_ALL, 1)
    ]
    count = len(relative)
    at = lax.axis_index(("zk", "zp"))
    return jnp.stack(
        [lax.select_n((place - at) % count, *relative) for place in range(count)], axis=1
    )


def gathered_y(block):
    pieces = [(0, 0, block)]
    half = block.shape[1] // 2
    up = down = block
    for k in range(1, 4):
        up = shifted(up, "y", 1)
        down = shifted(down, "y", -1)
        pieces += [(-k, 0, up), (k, 0, down)]
    pieces.append((4, 0, shifted(up[:, :half], "y", 1)))
    pieces.append((4, half, shifted(down[:, half:], "y", -1)))
    count, y_at = lax.axis_size("y"), lax.axis_index("y")
    parts, z_count, share, columns = block.shape
    whole = jnp.zeros((parts, z_count, count, share, columns), block.dtype)
    for k, first, piece in pieces:
        whole = lax.dynamic_update_slice(
            whole, piece[:, :, None], (0, first, (y_at + k) % count, 0, 0)
        )
    return whole.reshape(parts, -1, columns)


def gelu_parts(gate):
    normal_cdf = 0.5 * (1.0 + jax.scipy.special.erf(gate * (1.0 / math.sqrt(2.0))))
    density = jnp.exp(-0.5 * gate * gate) * (1.0 / math.sqrt(2.0 * math.pi))
    return (gate * normal_cdf, normal_cdf + gate * density)


def block_gradients(out_grad, gate_lin, up_lin, conv_weight, gate_weight, up_weight, down_weight):
    rows, columns = gate_lin.shape
    width = out_grad.shape[1]
    half = columns // 2
    second = lax.axis_index("zp") == 1

    own, other = halves_of(jnp.stack([down_weight.T, gate_weight, up_weight]), second)
    block = gathered_z(own, other)
    block, out_grad, gate_lin, up_lin = lax.optimization_barrier(
        (block, out_grad, gate_lin, up_lin)
    )
    down_full, gate_full, up_full = gathered_y(block)

    spare = ((0, 0), (0, columns - width))
    last = jnp.concatenate([gate_lin[-2:], up_lin[-1:], jnp.pad(out_grad[-1:], spare)])
    lead = jnp.concatenate([gate_lin[:2], up_lin[:1], jnp.pad(out_grad[:1], spare)])
    before = to_next(last, SEQ_AXES, 1)
    after = to_next(lead, SEQ_AXES, -1)
    grads = jnp.concatenate(
        [
            before[3:, :width],
            out_grad,
            after[3:, :width],
            jnp.zeros((PAD - rows - 2, width), out_grad.dtype),
        ]
    )
    grads = sent_to_all(grads, GROUP).reshape(2, -1, PAD, width)
    grads = grads.transpose(0, 2, 1, 3).reshape(2 * PAD, -1)

    saved = jnp.concatenate(
        [before[:2], gate_lin, after[:2], before[2:3], up_lin, after[2:3]]
    )
    kept, sent = halves_of(saved, second)
    came = swapped(sent, "zp", 1)
    pair = jnp.stack([jnp.where(second, came, kept), jnp.where(second, kept, came)])
    pair = pair.astype(jnp.float32)
    linear, up_ext = pair[:, : rows + 4], pair[:, rows + 4 :]
    start = lax.axis_index(TP) * columns + jnp.where(second, half, 0)
    taps = lax.dynamic_slice_in_dim(conv_weight, start, half, 1).astype(jnp.float32)

    gate = taps[0] * linear[:, :-2] + taps[1] * linear[:, 1:-1] + taps[2] * linear[:, 2:]
    gelu_value, gelu_slope = gelu_parts(gate)

    act_grad = jnp.dot(grads, down_full, preferred_element_type=jnp.float32)
    act_grad = act_grad.reshape(2, PAD, half)[:, : rows + 2]
    gate_grad = act_grad * up_ext * gelu_slope
    up_grad = (act_grad * gelu_value)[:, 1:-1].astype(jnp.bfloat16)
    own_grad = gate_grad[:, 1:-1]
    linear_grad = (
        taps[0] * gate_grad[:, 2:] + taps[1] * own_grad + taps[2] * gate_grad[:, :-2]
    ).astype(jnp.bfloat16)

    conv = jnp.stack(
        [jnp.sum(own_grad * linear[:, 1 + k : 1 + k + rows], axis=(0, 1)) for k in range(3)]
    )
    conv = sent_to_all(conv, Z_ALL)
    conv = conv.reshape(-1, 2, 3, half).sum(axis=0).transpose(1, 0, 2).reshape(3, columns)
    contract = (((1,), (1,)), ((), ()))
    product = lax.dot_general(
        linear_grad.reshape(-1, half), gate_full, contract, preferred_element_type=jnp.float32
    ) + lax.dot_general(
        up_grad.reshape(-1, half), up_full, contract, preferred_element_type=jnp.float32
    )
    product = product.astype(jnp.bfloat16).reshape(2, rows, -1, width)
    product = product.transpose(0, 2, 1, 3).reshape(-1, rows, width)
    conv, product = lax.optimization_barrier((conv, product))
    arrived = lax.all_to_all(product, GROUP, 0, 0, tiled=True)
    input_grad = arrived.astype(jnp.float32).sum(axis=0).astype(jnp.bfloat16)
    for bit in (1, 2, 4):
        conv = conv + swapped(conv, "y", bit)
    conv = conv[None]
    for axis, bit in (("core", 1), ("x", 1), ("x", 2)):
        low = lax.axis_index(axis) & bit == 0
        peer = swapped(conv, axis, bit)
        conv = jnp.concatenate([jnp.where(low, conv, peer), jnp.where(low, peer, conv)])
    conv_grad = conv.transpose(1, 0, 2).reshape(3, -1)
    return (input_grad, conv_grad)


def solution(mesh):
    finer = Mesh(
        mesh.devices.reshape(mesh.shape["rep"], 2, 2, 8, 4, 2),
        ("rep", "zk", "zp", "y", "x", "core"),
    )
    return jax.shard_map(
        block_gradients,
        mesh=finer,
        in_specs=(
            P(ROWS, TP),
            P(ROWS, TP),
            P(ROWS, TP),
            P(),
            P(SEQ_AXES, TP),
            P(SEQ_AXES, TP),
            P(TP, SEQ_AXES),
        ),
        out_specs=(P(ROWS, TP), P()),
        check_vma=False,
    )
```

```python
import math

import jax
import jax.numpy as jnp
from jax import lax
from jax.experimental import pallas as pl
from jax.experimental.pallas import tpu as pltpu
from jax.sharding import Mesh
from jax.sharding import PartitionSpec as P


Z_ALL = ("rep", "zk", "zp")
SEQ_AXES = ("zk", "zp", "y")
TP = ("x", "core")
GROUP = ("zp", "x", "core")
ROWS = ("rep", "zk", "zp", "y")
PAD = 264


def shifted(value, axis, by):
    count = lax.axis_size(axis)
    return lax.ppermute(value, axis, [(i, (i + by) % count) for i in range(count)])


def to_next(value, axis, by):
    count = lax.axis_size(axis)
    pairs = [(i, i + by) for i in range(count) if 0 <= i + by < count]
    return lax.ppermute(value, axis, pairs)


def swapped(value, axis, bit):
    return lax.ppermute(value, axis, [(i, i ^ bit) for i in range(lax.axis_size(axis))])


def sent_to_all(value, axis):
    peers = lax.axis_size(axis)
    return lax.all_to_all(
        jnp.broadcast_to(value[None], (peers, *value.shape)), axis, 0, 0, tiled=True
    )


def halves_of(value, second):
    half = value.shape[-1] // 2
    left, right = value[..., :half], value[..., half:]
    return jnp.where(second, right, left), jnp.where(second, left, right)


def gathered_z(own, other):
    relative = [own, shifted(other, Z_ALL, -1), shifted(own, Z_ALL, 2), shifted(other, Z_ALL, 1)]
    count = len(relative)
    at = lax.axis_index(("zk", "zp"))
    return jnp.stack(
        [lax.select_n((place - at) % count, *relative) for place in range(count)], axis=1
    )


def gathered_y(block):
    count, y_at = lax.axis_size("y"), lax.axis_index("y")
    parts, z_count, share, columns = block.shape
    whole = jnp.zeros((parts, z_count, count, share, columns), block.dtype)
    block, whole = lax.optimization_barrier((block, whole))
    pieces = [(0, 0, block)]
    half = block.shape[1] // 2
    up = down = block
    for k in range(1, 4):
        up = shifted(up, "y", 1)
        down = shifted(down, "y", -1)
        pieces += [(-k, 0, up), (k, 0, down)]
    pieces.append((4, 0, shifted(up[:, :half], "y", 1)))
    pieces.append((4, half, shifted(down[:, half:], "y", -1)))
    for k, first, piece in pieces:
        whole = lax.dynamic_update_slice(
            whole, piece[:, :, None], (0, first, (y_at + k) % count, 0, 0)
        )
    return whole.reshape(parts, -1, columns)


def gelu_parts(gate):
    normal_cdf = 0.5 * (1.0 + jax.scipy.special.erf(gate * (1.0 / math.sqrt(2.0))))
    density = jnp.exp(-0.5 * gate * gate) * (1.0 / math.sqrt(2.0 * math.pi))
    return (gate * normal_cdf, normal_cdf + gate * density)


def hidden_kernel(grads, down, slope, value, linear, taps, linear_out, up_out, conv_out):
    peers, padded, width = grads.shape
    rows = linear_out.shape[1]
    act = jnp.zeros(slope.shape[1:], jnp.float32)
    for t in range(peers):
        act += jnp.dot(
            grads[t], down[0, t * width : (t + 1) * width], preferred_element_type=jnp.float32
        )
    grad = act * slope[0]

    def ahead(value, by):
        return pltpu.roll(value, padded - by, 0)

    linear_grad = (
        taps[0:1] * ahead(grad, 2) + taps[1:2] * ahead(grad, 1) + taps[2:3] * grad
    )
    linear_out[0] = linear_grad[:rows].astype(jnp.bfloat16)
    up_out[0] = ahead(act * value[0], 1)[:rows].astype(jnp.bfloat16)
    at = lax.broadcasted_iota(jnp.int32, grad.shape, 0)
    own = jnp.where((at >= 1) & (at <= rows), grad, 0.0)
    near = linear[0]
    sums = jnp.concatenate(
        [
            jnp.sum(own * (near if k == 0 else ahead(near, k)), axis=0, keepdims=True)
            for k in range(3)
        ]
    )
    first = pl.program_id(0) == 0

    @pl.when(first)
    def _():
        conv_out[...] = sums

    @pl.when(jnp.logical_not(first))
    def _():
        conv_out[...] += sums


def hidden_gradients(grads, weights, slope, value, linear, taps):
    peers, padded, width = grads.shape
    _, depth, half = weights.shape
    rows = width
    saved = pl.BlockSpec((1, padded, half), lambda b: (b, 0, 0))
    made = pl.BlockSpec((1, rows, half), lambda b: (b, 0, 0))
    return pl.pallas_call(
        hidden_kernel,
        grid=(2,),
        in_specs=[
            pl.BlockSpec((peers // 2, padded, width), lambda b: (b, 0, 0)),
            pl.BlockSpec((1, depth, half), lambda b: (0, 0, 0)),
            saved,
            saved,
            saved,
            pl.BlockSpec((3, half), lambda b: (0, 0)),
        ],
        out_specs=[made, made, pl.BlockSpec((3, half), lambda b: (0, 0))],
        out_shape=[
            jax.ShapeDtypeStruct((2, rows, half), jnp.bfloat16),
            jax.ShapeDtypeStruct((2, rows, half), jnp.bfloat16),
            jax.ShapeDtypeStruct((3, half), jnp.float32),
        ],
    )(grads, weights, slope, value, linear, taps)


def output_kernel(linear_grad, up_grad, gate, up, out):
    width = out.shape[3]
    contract = (((1,), (1,)), ((), ()))
    for t in range(out.shape[1]):
        span = slice(t * width, (t + 1) * width)
        for b in range(2):
            part = lax.dot_general(
                linear_grad[b], gate[0, span], contract, preferred_element_type=jnp.float32
            ) + lax.dot_general(
                up_grad[b], up[0, span], contract, preferred_element_type=jnp.float32
            )
            out[b, t] = part.astype(jnp.bfloat16)


def output_partials(linear_grad, up_grad, weights, width):
    _, rows, half = linear_grad.shape
    peers = weights.shape[1] // width
    steps = 4
    whole = pl.BlockSpec((2, rows, half), lambda i: (0, 0, 0))
    product = pl.pallas_call(
        output_kernel,
        grid=(steps,),
        in_specs=[
            whole,
            whole,
            pl.BlockSpec((1, weights.shape[1] // steps, half), lambda i: (1, i, 0)),
            pl.BlockSpec((1, weights.shape[1] // steps, half), lambda i: (2, i, 0)),
        ],
        out_specs=pl.BlockSpec((2, peers // steps, rows, width), lambda i: (0, i, 0, 0)),
        out_shape=jax.ShapeDtypeStruct((2, peers, rows, width), jnp.bfloat16),
    )(linear_grad, up_grad, weights, weights)
    return product.reshape(2 * peers, rows, width)


def block_gradients(out_grad, gate_lin, up_lin, conv_weight, gate_weight, up_weight, down_weight):
    rows, columns = gate_lin.shape
    width = out_grad.shape[1]
    half = columns // 2
    second = lax.axis_index("zp") == 1

    own, other = halves_of(jnp.stack([down_weight.T, gate_weight, up_weight]), second)
    weights = gathered_y(gathered_z(own, other))

    spare = ((0, 0), (0, columns - width))
    last = jnp.concatenate([gate_lin[-2:], up_lin[-1:], jnp.pad(out_grad[-1:], spare)])
    lead = jnp.concatenate([gate_lin[:2], up_lin[:1], jnp.pad(out_grad[:1], spare)])
    before = to_next(last, SEQ_AXES, 1)
    after = to_next(lead, SEQ_AXES, -1)
    grads = jnp.concatenate(
        [
            before[3:, :width],
            out_grad,
            after[3:, :width],
            jnp.zeros((PAD - rows - 2, width), out_grad.dtype),
        ]
    )
    grads = sent_to_all(grads, GROUP)

    saved = jnp.concatenate(
        [before[:2], gate_lin, after[:2], before[2:3], up_lin, after[2:3]]
    )
    kept, sent = halves_of(saved, second)
    came = swapped(sent, "zp", 1)
    pair = jnp.stack([jnp.where(second, came, kept), jnp.where(second, kept, came)])
    pair = pair.astype(jnp.float32)
    linear, up_ext = pair[:, : rows + 4], pair[:, rows + 4 :]
    start = lax.axis_index(TP) * columns + jnp.where(second, half, 0)
    taps = lax.dynamic_slice_in_dim(conv_weight, start, half, 1).astype(jnp.float32)

    gate = taps[0] * linear[:, :-2] + taps[1] * linear[:, 1:-1] + taps[2] * linear[:, 2:]
    gelu_value, gelu_slope = gelu_parts(gate)

    tail = ((0, 0), (0, PAD - rows - 2), (0, 0))
    linear_grad, up_grad, conv = hidden_gradients(
        grads,
        weights,
        jnp.pad(up_ext * gelu_slope, tail),
        jnp.pad(gelu_value, tail),
        jnp.pad(linear, ((0, 0), (0, PAD - rows - 4), (0, 0))),
        taps,
    )
    one, two = shifted(conv, "rep", 1), shifted(conv, "rep", 2)
    product = output_partials(linear_grad, up_grad, weights, width)
    arrived = lax.all_to_all(product, GROUP, 0, 0, tiled=True)
    input_grad = arrived.astype(jnp.float32).sum(axis=0).astype(jnp.bfloat16)
    rep_at, rep_count = lax.axis_index("rep"), lax.axis_size("rep")
    conv = sum(lax.select_n((rep_at - k) % rep_count, conv, one, two) for k in range(rep_count))
    near = conv + swapped(conv, "zk", 1)
    pair_swap = [(i, i ^ 1) for i in range(4)]
    both_swap = [(i, i ^ 3) for i in range(4)]
    far = lax.ppermute(conv, ("zk", "zp"), pair_swap) + lax.ppermute(conv, ("zk", "zp"), both_swap)
    conv = jnp.concatenate(
        [jnp.where(second, far, near), jnp.where(second, near, far)], axis=1
    )
    conv = (conv + swapped(conv, "y", 1)) + (swapped(conv, "y", 2) + swapped(conv, "y", 3))
    conv = conv + swapped(conv, "y", 4)
    low = lax.axis_index("core") == 0
    peer = swapped(conv, "core", 1)
    conv = jnp.stack([jnp.where(low, conv, peer), jnp.where(low, peer, conv)])
    peers = [conv] + [swapped(conv, "x", k) for k in range(1, 4)]
    x_at = lax.axis_index("x")
    conv = jnp.concatenate([lax.select_n(x_at ^ k, *peers) for k in range(4)])
    conv_grad = conv.transpose(1, 0, 2).reshape(3, -1)
    return (input_grad, conv_grad)


def solution(mesh):
    finer = Mesh(
        mesh.devices.reshape(mesh.shape["rep"], 2, 2, 8, 4, 2),
        ("rep", "zk", "zp", "y", "x", "core"),
    )
    return jax.shard_map(
        block_gradients,
        mesh=finer,
        in_specs=(
            P(ROWS, TP),
            P(ROWS, TP),
            P(ROWS, TP),
            P(),
            P(SEQ_AXES, TP),
            P(SEQ_AXES, TP),
            P(TP, SEQ_AXES),
        ),
        out_specs=(P(ROWS, TP), P()),
        check_vma=False,
    )
```

```python
import math

import jax
import jax.numpy as jnp
from jax import lax
from jax.experimental import pallas as pl
from jax.experimental.pallas import tpu as pltpu
from jax.sharding import Mesh
from jax.sharding import PartitionSpec as P


Z_ALL = ("rep", "zk", "zp")
SEQ_AXES = ("zk", "zp", "y")
TP = ("x", "core")
GROUP = ("zp", "x", "core")
ROWS = ("rep", "zk", "zp", "y")
PAD = 264


def shifted(value, axis, by):
    count = lax.axis_size(axis)
    return lax.ppermute(value, axis, [(i, (i + by) % count) for i in range(count)])


def to_next(value, axis, by):
    count = lax.axis_size(axis)
    pairs = [(i, i + by) for i in range(count) if 0 <= i + by < count]
    return lax.ppermute(value, axis, pairs)


def swapped(value, axis, bit):
    return lax.ppermute(value, axis, [(i, i ^ bit) for i in range(lax.axis_size(axis))])


def sent_to_all(value, axis):
    peers = lax.axis_size(axis)
    return lax.all_to_all(
        jnp.broadcast_to(value[None], (peers, *value.shape)), axis, 0, 0, tiled=True
    )


def halves_of(value, second):
    half = value.shape[-1] // 2
    left, right = value[..., :half], value[..., half:]
    return jnp.where(second, right, left), jnp.where(second, left, right)


def gathered_z(own, other):
    relative = [own, shifted(other, Z_ALL, -1), shifted(own, Z_ALL, 2), shifted(other, Z_ALL, 1)]
    count = len(relative)
    at = lax.axis_index(("zk", "zp"))
    return jnp.stack(
        [lax.select_n((place - at) % count, *relative) for place in range(count)], axis=1
    )


def gathered_y(block):
    half = block.shape[1] // 2
    pieces = {0: block}
    up = down = block
    for k in range(1, 4):
        up = shifted(up, "y", 1)
        down = shifted(down, "y", -1)
        pieces[-k], pieces[k] = up, down
    ends = [(0, shifted(up[:, :half], "y", 1)), (half, shifted(down[:, half:], "y", -1))]
    count, y_at = lax.axis_size("y"), lax.axis_index("y")
    parts, z_count, share, columns = block.shape
    base = -2
    whole = jnp.broadcast_to(
        pieces[base][:, :, None], (parts, z_count, count, share, columns)
    )
    placed = [(k, 0, piece) for k, piece in pieces.items() if k != base]
    for k, first, piece in placed + [(4, first, piece) for first, piece in ends]:
        whole = lax.dynamic_update_slice(
            whole, piece[:, :, None], (0, first, (y_at + k) % count, 0, 0)
        )
    return whole.reshape(parts, -1, columns), pieces[3]


def gelu_parts(gate):
    normal_cdf = 0.5 * (1.0 + jax.scipy.special.erf(gate * (1.0 / math.sqrt(2.0))))
    density = jnp.exp(-0.5 * gate * gate) * (1.0 / math.sqrt(2.0 * math.pi))
    return (gate * normal_cdf, normal_cdf + gate * density)


def hidden_kernel(grads, down, slope, value, linear, taps, linear_out, up_out, conv_out):
    peers, padded, width = grads.shape
    rows = linear_out.shape[1]
    act = jnp.zeros(slope.shape[1:], jnp.float32)
    for t in range(peers):
        act += jnp.dot(
            grads[t], down[0, t * width : (t + 1) * width], preferred_element_type=jnp.float32
        )
    grad = act * slope[0]

    def ahead(value, by):
        return pltpu.roll(value, padded - by, 0)

    linear_grad = (
        taps[0:1] * ahead(grad, 2) + taps[1:2] * ahead(grad, 1) + taps[2:3] * grad
    )
    linear_out[0] = linear_grad[:rows].astype(jnp.bfloat16)
    up_out[0] = ahead(act * value[0], 1)[:rows].astype(jnp.bfloat16)
    at = lax.broadcasted_iota(jnp.int32, grad.shape, 0)
    own = jnp.where((at >= 1) & (at <= rows), grad, 0.0)
    near = linear[0]
    sums = jnp.concatenate(
        [
            jnp.sum(own * (near if k == 0 else ahead(near, k)), axis=0, keepdims=True)
            for k in range(3)
        ]
    )
    first = pl.program_id(0) == 0

    @pl.when(first)
    def _():
        conv_out[...] = sums

    @pl.when(jnp.logical_not(first))
    def _():
        conv_out[...] += sums


def hidden_gradients(grads, weights, slope, value, linear, taps):
    peers, padded, width = grads.shape
    _, depth, half = weights.shape
    rows = width
    saved = pl.BlockSpec((1, padded, half), lambda b: (b, 0, 0))
    made = pl.BlockSpec((1, rows, half), lambda b: (b, 0, 0))
    return pl.pallas_call(
        hidden_kernel,
        grid=(2,),
        in_specs=[
            pl.BlockSpec((peers // 2, padded, width), lambda b: (b, 0, 0)),
            pl.BlockSpec((1, depth, half), lambda b: (0, 0, 0)),
            saved,
            saved,
            saved,
            pl.BlockSpec((3, half), lambda b: (0, 0)),
        ],
        out_specs=[made, made, pl.BlockSpec((3, half), lambda b: (0, 0))],
        out_shape=[
            jax.ShapeDtypeStruct((2, rows, half), jnp.bfloat16),
            jax.ShapeDtypeStruct((2, rows, half), jnp.bfloat16),
            jax.ShapeDtypeStruct((3, half), jnp.float32),
        ],
    )(grads, weights, slope, value, linear, taps)


def output_kernel(linear_grad, up_grad, gate, up, out):
    width = out.shape[3]
    contract = (((1,), (1,)), ((), ()))
    for t in range(out.shape[1]):
        span = slice(t * width, (t + 1) * width)
        for b in range(2):
            part = lax.dot_general(
                linear_grad[b], gate[0, span], contract, preferred_element_type=jnp.float32
            ) + lax.dot_general(
                up_grad[b], up[0, span], contract, preferred_element_type=jnp.float32
            )
            out[b, t] = part.astype(jnp.bfloat16)


def output_partials(linear_grad, up_grad, weights, width):
    _, rows, half = linear_grad.shape
    peers = weights.shape[1] // width
    steps = 4
    whole = pl.BlockSpec((2, rows, half), lambda i: (0, 0, 0))
    product = pl.pallas_call(
        output_kernel,
        grid=(steps,),
        in_specs=[
            whole,
            whole,
            pl.BlockSpec((1, weights.shape[1] // steps, half), lambda i: (1, i, 0)),
            pl.BlockSpec((1, weights.shape[1] // steps, half), lambda i: (2, i, 0)),
        ],
        out_specs=pl.BlockSpec((2, peers // steps, rows, width), lambda i: (0, i, 0, 0)),
        out_shape=jax.ShapeDtypeStruct((2, peers, rows, width), jnp.bfloat16),
    )(linear_grad, up_grad, weights, weights)
    return product.reshape(2 * peers, rows, width)


def block_gradients(out_grad, gate_lin, up_lin, conv_weight, gate_weight, up_weight, down_weight):
    rows, columns = gate_lin.shape
    width = out_grad.shape[1]
    half = columns // 2
    second = lax.axis_index("zp") == 1

    own, other = halves_of(jnp.stack([down_weight.T, gate_weight, up_weight]), second)
    weights, late = gathered_y(gathered_z(own, other))

    spare = ((0, 0), (0, columns - width))
    last = jnp.concatenate([gate_lin[-2:], up_lin[-1:], jnp.pad(out_grad[-1:], spare)])
    lead = jnp.concatenate([gate_lin[:2], up_lin[:1], jnp.pad(out_grad[:1], spare)])
    before = to_next(last, SEQ_AXES, 1)
    after = to_next(lead, SEQ_AXES, -1)
    grads = jnp.concatenate(
        [
            before[3:, :width],
            out_grad,
            after[3:, :width],
            jnp.zeros((PAD - rows - 2, width), out_grad.dtype),
        ]
    )
    grads = sent_to_all(grads, GROUP)

    kept, sent = halves_of(jnp.concatenate([gate_lin, up_lin, before, after]), second)
    came = swapped(sent, "zp", 1)
    kept, came, _ = lax.optimization_barrier((kept, came, late))
    pair = jnp.stack([jnp.where(second, came, kept), jnp.where(second, kept, came)])
    pair = pair.astype(jnp.float32)
    edge = pair[:, 2 * rows :]
    linear = jnp.concatenate([edge[:, :2], pair[:, :rows], edge[:, 4:6]], axis=1)
    up_ext = jnp.concatenate([edge[:, 2:3], pair[:, rows : 2 * rows], edge[:, 6:7]], axis=1)
    start = lax.axis_index(TP) * columns + jnp.where(second, half, 0)
    taps = lax.dynamic_slice_in_dim(conv_weight, start, half, 1).astype(jnp.float32)

    gate = taps[0] * linear[:, :-2] + taps[1] * linear[:, 1:-1] + taps[2] * linear[:, 2:]
    gelu_value, gelu_slope = gelu_parts(gate)

    tail = ((0, 0), (0, PAD - rows - 2), (0, 0))
    linear_grad, up_grad, conv = hidden_gradients(
        grads,
        weights,
        jnp.pad(up_ext * gelu_slope, tail),
        jnp.pad(gelu_value, tail),
        jnp.pad(linear, ((0, 0), (0, PAD - rows - 4), (0, 0))),
        taps,
    )
    conv = sent_to_all(conv, Z_ALL)
    conv = conv.reshape(-1, 2, 3, half).sum(axis=0).transpose(1, 0, 2).reshape(3, columns)
    product = output_partials(linear_grad, up_grad, weights, width)
    arrived = lax.all_to_all(product, GROUP, 0, 0, tiled=True)
    input_grad = arrived.astype(jnp.float32).sum(axis=0).astype(jnp.bfloat16)
    for bit in (1, 2, 4):
        conv = conv + swapped(conv, "y", bit)
    conv = conv[None]
    for axis, bit in (("core", 1), ("x", 1), ("x", 2)):
        low = lax.axis_index(axis) & bit == 0
        peer = swapped(conv, axis, bit)
        conv = jnp.concatenate([jnp.where(low, conv, peer), jnp.where(low, peer, conv)])
    conv_grad = conv.transpose(1, 0, 2).reshape(3, -1)
    return (input_grad, conv_grad)


def solution(mesh):
    finer = Mesh(
        mesh.devices.reshape(mesh.shape["rep"], 2, 2, 8, 4, 2),
        ("rep", "zk", "zp", "y", "x", "core"),
    )
    return jax.shard_map(
        block_gradients,
        mesh=finer,
        in_specs=(
            P(ROWS, TP),
            P(ROWS, TP),
            P(ROWS, TP),
            P(),
            P(SEQ_AXES, TP),
            P(SEQ_AXES, TP),
            P(TP, SEQ_AXES),
        ),
        out_specs=(P(ROWS, TP), P()),
        check_vma=False,
    )
```

```python
import math

import jax
import jax.numpy as jnp
from jax import lax
from jax.experimental import pallas as pl
from jax.experimental.pallas import tpu as pltpu
from jax.sharding import Mesh
from jax.sharding import PartitionSpec as P


Z_ALL = ("rep", "zk", "zp")
SEQ_AXES = ("zk", "zp", "y")
TP = ("x", "core")
GROUP = ("zp", "x", "core")
ROWS = ("rep", "zk", "zp", "y")
PAD = 264


def shifted(value, axis, by):
    count = lax.axis_size(axis)
    return lax.ppermute(value, axis, [(i, (i + by) % count) for i in range(count)])


def to_next(value, axis, by):
    count = lax.axis_size(axis)
    pairs = [(i, i + by) for i in range(count) if 0 <= i + by < count]
    return lax.ppermute(value, axis, pairs)


def swapped(value, axis, bit):
    return lax.ppermute(value, axis, [(i, i ^ bit) for i in range(lax.axis_size(axis))])


def sent_to_all(value, axis):
    peers = lax.axis_size(axis)
    return lax.all_to_all(
        jnp.broadcast_to(value[None], (peers, *value.shape)), axis, 0, 0, tiled=True
    )


def halves_of(value, second):
    half = value.shape[-1] // 2
    left, right = value[..., :half], value[..., half:]
    return jnp.where(second, right, left), jnp.where(second, left, right)


def gathered_z(own, other):
    relative = [own, shifted(other, Z_ALL, -1), shifted(own, Z_ALL, 2), shifted(other, Z_ALL, 1)]
    count = len(relative)
    at = lax.axis_index(("zk", "zp"))
    return jnp.stack(
        [lax.select_n((place - at) % count, *relative) for place in range(count)], axis=1
    )


def placed(pieces, base, count, y_at):
    first = pieces.pop(base)[0][1]
    outer, share, columns = first.shape
    whole = jnp.broadcast_to(first[:, None], (outer, count, share, columns))
    for k, parts in pieces.items():
        for start, part in parts:
            whole = lax.dynamic_update_slice(whole, part[:, None], (start, (y_at + k) % count, 0, 0))
    return whole


def gathered_y(block):
    _, z_count, share, columns = block.shape
    own_down, own_rest = block[0], block[1:].reshape(-1, share, columns)
    rest, mid = own_rest.shape[0], z_count // 2
    downs, rests = {0: [(0, own_down)]}, {0: [(0, own_rest)]}
    up, low = shifted(own_down, "y", 1), shifted(own_down, "y", -1)
    downs[-1], downs[1] = [(0, up)], [(0, low)]
    up = jnp.concatenate([own_rest, up])
    low = jnp.concatenate([own_rest, low[mid:], low[:mid]])
    for k in (2, 3):
        up, low = shifted(up, "y", 1), shifted(low, "y", -1)
        downs[-k] = [(0, up[rest:])]
        downs[k] = [(mid, low[rest : rest + mid]), (0, low[rest + mid :])]
        rests[1 - k], rests[k - 1] = [(0, up[:rest])], [(0, low[:rest])]
    late = low
    up, low = shifted(up[: rest + mid], "y", 1), shifted(low[: rest + mid], "y", -1)
    downs[4] = [(0, up[rest:]), (mid, low[rest:])]
    rests[-3], rests[3] = [(0, up[:rest])], [(0, low[:rest])]
    rests[4] = [(0, shifted(up[:z_count], "y", 1)), (z_count, shifted(low[z_count:rest], "y", -1))]
    count, y_at = lax.axis_size("y"), lax.axis_index("y")
    down_full = placed(downs, -1, count, y_at).reshape(1, -1, columns)
    rest_full = placed(rests, -1, count, y_at).reshape(rest // z_count, -1, columns)
    return down_full, rest_full, late


def gelu_parts(gate):
    normal_cdf = 0.5 * (1.0 + jax.scipy.special.erf(gate * (1.0 / math.sqrt(2.0))))
    density = jnp.exp(-0.5 * gate * gate) * (1.0 / math.sqrt(2.0 * math.pi))
    return (gate * normal_cdf, normal_cdf + gate * density)


def hidden_kernel(grads, down, slope, value, linear, taps, linear_out, up_out, conv_out):
    peers, padded, width = grads.shape
    rows = linear_out.shape[1]
    act = jnp.zeros(slope.shape[1:], jnp.float32)
    for t in range(peers):
        act += jnp.dot(
            grads[t], down[0, t * width : (t + 1) * width], preferred_element_type=jnp.float32
        )
    grad = act * slope[0]

    def ahead(value, by):
        return pltpu.roll(value, padded - by, 0)

    linear_grad = (
        taps[0:1] * ahead(grad, 2) + taps[1:2] * ahead(grad, 1) + taps[2:3] * grad
    )
    linear_out[0] = linear_grad[:rows].astype(jnp.bfloat16)
    up_out[0] = ahead(act * value[0], 1)[:rows].astype(jnp.bfloat16)
    at = lax.broadcasted_iota(jnp.int32, grad.shape, 0)
    own = jnp.where((at >= 1) & (at <= rows), grad, 0.0)
    near = linear[0]
    sums = jnp.concatenate(
        [
            jnp.sum(own * (near if k == 0 else ahead(near, k)), axis=0, keepdims=True)
            for k in range(3)
        ]
    )
    first = pl.program_id(0) == 0

    @pl.when(first)
    def _():
        conv_out[...] = sums

    @pl.when(jnp.logical_not(first))
    def _():
        conv_out[...] += sums


def hidden_gradients(grads, weights, slope, value, linear, taps):
    peers, padded, width = grads.shape
    _, depth, half = weights.shape
    rows = width
    saved = pl.BlockSpec((1, padded, half), lambda b: (b, 0, 0))
    made = pl.BlockSpec((1, rows, half), lambda b: (b, 0, 0))
    return pl.pallas_call(
        hidden_kernel,
        grid=(2,),
        in_specs=[
            pl.BlockSpec((peers // 2, padded, width), lambda b: (b, 0, 0)),
            pl.BlockSpec((1, depth, half), lambda b: (0, 0, 0)),
            saved,
            saved,
            saved,
            pl.BlockSpec((3, half), lambda b: (0, 0)),
        ],
        out_specs=[made, made, pl.BlockSpec((3, half), lambda b: (0, 0))],
        out_shape=[
            jax.ShapeDtypeStruct((2, rows, half), jnp.bfloat16),
            jax.ShapeDtypeStruct((2, rows, half), jnp.bfloat16),
            jax.ShapeDtypeStruct((3, half), jnp.float32),
        ],
    )(grads, weights, slope, value, linear, taps)


def output_kernel(linear_grad, up_grad, gate, up, out):
    width = out.shape[3]
    contract = (((1,), (1,)), ((), ()))
    for t in range(out.shape[1]):
        span = slice(t * width, (t + 1) * width)
        for b in range(2):
            part = lax.dot_general(
                linear_grad[b], gate[0, span], contract, preferred_element_type=jnp.float32
            ) + lax.dot_general(
                up_grad[b], up[0, span], contract, preferred_element_type=jnp.float32
            )
            out[b, t] = part.astype(jnp.bfloat16)


def output_partials(linear_grad, up_grad, weights, width):
    _, rows, half = linear_grad.shape
    peers = weights.shape[1] // width
    steps = 4
    whole = pl.BlockSpec((2, rows, half), lambda i: (0, 0, 0))
    product = pl.pallas_call(
        output_kernel,
        grid=(steps,),
        in_specs=[
            whole,
            whole,
            pl.BlockSpec((1, weights.shape[1] // steps, half), lambda i: (0, i, 0)),
            pl.BlockSpec((1, weights.shape[1] // steps, half), lambda i: (1, i, 0)),
        ],
        out_specs=pl.BlockSpec((2, peers // steps, rows, width), lambda i: (0, i, 0, 0)),
        out_shape=jax.ShapeDtypeStruct((2, peers, rows, width), jnp.bfloat16),
    )(linear_grad, up_grad, weights, weights)
    return product.reshape(2 * peers, rows, width)


def block_gradients(out_grad, gate_lin, up_lin, conv_weight, gate_weight, up_weight, down_weight):
    rows, columns = gate_lin.shape
    width = out_grad.shape[1]
    half = columns // 2
    second = lax.axis_index("zp") == 1

    own, other = halves_of(jnp.stack([down_weight.T, gate_weight, up_weight]), second)
    down_full, rest_full, late = gathered_y(gathered_z(own, other))

    spare = ((0, 0), (0, columns - width))
    last = jnp.concatenate([gate_lin[-2:], up_lin[-1:], jnp.pad(out_grad[-1:], spare)])
    lead = jnp.concatenate([gate_lin[:2], up_lin[:1], jnp.pad(out_grad[:1], spare)])
    before = to_next(last, SEQ_AXES, 1)
    after = to_next(lead, SEQ_AXES, -1)
    grads = jnp.concatenate(
        [
            before[3:, :width],
            out_grad,
            after[3:, :width],
            jnp.zeros((PAD - rows - 2, width), out_grad.dtype),
        ]
    )
    grads = sent_to_all(grads, GROUP)

    kept, sent = halves_of(jnp.concatenate([gate_lin, up_lin, before, after]), second)
    came = swapped(sent, "zp", 1)
    kept, came, _ = lax.optimization_barrier((kept, came, late))
    pair = jnp.stack([jnp.where(second, came, kept), jnp.where(second, kept, came)])
    pair = pair.astype(jnp.float32)
    edge = pair[:, 2 * rows :]
    linear = jnp.concatenate([edge[:, :2], pair[:, :rows], edge[:, 4:6]], axis=1)
    up_ext = jnp.concatenate([edge[:, 2:3], pair[:, rows : 2 * rows], edge[:, 6:7]], axis=1)
    start = lax.axis_index(TP) * columns + jnp.where(second, half, 0)
    taps = lax.dynamic_slice_in_dim(conv_weight, start, half, 1).astype(jnp.float32)

    gate = taps[0] * linear[:, :-2] + taps[1] * linear[:, 1:-1] + taps[2] * linear[:, 2:]
    gelu_value, gelu_slope = gelu_parts(gate)

    tail = ((0, 0), (0, PAD - rows - 2), (0, 0))
    linear_grad, up_grad, conv = hidden_gradients(
        grads,
        down_full,
        jnp.pad(up_ext * gelu_slope, tail),
        jnp.pad(gelu_value, tail),
        jnp.pad(linear, ((0, 0), (0, PAD - rows - 4), (0, 0))),
        taps,
    )
    conv = sent_to_all(conv, Z_ALL)
    conv = conv.reshape(-1, 2, 3, half).sum(axis=0).transpose(1, 0, 2).reshape(3, columns)
    product = output_partials(linear_grad, up_grad, rest_full, width)
    arrived = lax.all_to_all(product, GROUP, 0, 0, tiled=True)
    input_grad = arrived.astype(jnp.float32).sum(axis=0).astype(jnp.bfloat16)
    for bit in (1, 2, 4):
        conv = conv + swapped(conv, "y", bit)
    conv = conv[None]
    for axis, bit in (("core", 1), ("x", 1), ("x", 2)):
        low = lax.axis_index(axis) & bit == 0
        peer = swapped(conv, axis, bit)
        conv = jnp.concatenate([jnp.where(low, conv, peer), jnp.where(low, peer, conv)])
    conv_grad = conv.transpose(1, 0, 2).reshape(3, -1)
    return (input_grad, conv_grad)


def solution(mesh):
    finer = Mesh(
        mesh.devices.reshape(mesh.shape["rep"], 2, 2, 8, 4, 2),
        ("rep", "zk", "zp", "y", "x", "core"),
    )
    return jax.shard_map(
        block_gradients,
        mesh=finer,
        in_specs=(
            P(ROWS, TP),
            P(ROWS, TP),
            P(ROWS, TP),
            P(),
            P(SEQ_AXES, TP),
            P(SEQ_AXES, TP),
            P(TP, SEQ_AXES),
        ),
        out_specs=(P(ROWS, TP), P()),
        check_vma=False,
    )
```

```python
import math

import jax
import jax.numpy as jnp
from jax import lax
from jax.experimental import pallas as pl
from jax.experimental.pallas import tpu as pltpu
from jax.sharding import Mesh
from jax.sharding import PartitionSpec as P


Z_ALL = ("rep", "zk", "zp")
SEQ_AXES = ("zk", "zp", "y")
TP = ("x", "core")
GROUP = ("zp", "x", "core")
ROWS = ("rep", "zk", "zp", "y")
PAD = 264
PIECES = 9


def shifted(value, axis, by):
    count = lax.axis_size(axis)
    return lax.ppermute(value, axis, [(i, (i + by) % count) for i in range(count)])


def to_next(value, axis, by):
    count = lax.axis_size(axis)
    pairs = [(i, i + by) for i in range(count) if 0 <= i + by < count]
    return lax.ppermute(value, axis, pairs)


def swapped(value, axis, bit):
    return lax.ppermute(value, axis, [(i, i ^ bit) for i in range(lax.axis_size(axis))])


def sent_to_all(value, axis):
    peers = lax.axis_size(axis)
    return lax.all_to_all(
        jnp.broadcast_to(value[None], (peers, *value.shape)), axis, 0, 0, tiled=True
    )


def halves_of(value, second):
    half = value.shape[-1] // 2
    left, right = value[..., :half], value[..., half:]
    return jnp.where(second, right, left), jnp.where(second, left, right)


def crossed(value, axis, by):
    names = axis if isinstance(axis, tuple) else (axis,)
    count = lax.axis_size(names)
    pairs = [
        (2 * i + core, 2 * ((i + step) % count) + core)
        for i in range(count)
        for core, step in enumerate((by, -by))
    ]
    return lax.ppermute(value, (*names, "core"), pairs)


def gathered_z(own, other):
    relative = [own, shifted(other, Z_ALL, -1), crossed(own, Z_ALL, 2), shifted(other, Z_ALL, 1)]
    count = len(relative)
    at = lax.axis_index(("zk", "zp"))
    return jnp.stack([lax.select_n((place - at) % count, *relative) for place in range(count)])


def gathered_y(block):
    mid = block.shape[0] // 2
    pieces, steps = [block], [0]
    one = two = block
    for k in range(1, 4):
        one, two = crossed(one, "y", 1), crossed(two, "y", -1)
        pieces += [one, two]
        steps += [-k, k]
    pieces += [crossed(one[:mid], "y", 1), crossed(two[mid:], "y", -1)]
    sign = 1 - 2 * lax.axis_index("core")
    count = lax.axis_size("y")
    places = (lax.axis_index("y") + sign * jnp.array(steps + [4, 4], jnp.int32)) % count
    return pieces, places.astype(jnp.int32), one


def gelu_parts(gate):
    normal_cdf = 0.5 * (1.0 + jax.scipy.special.erf(gate * (1.0 / math.sqrt(2.0))))
    density = jnp.exp(-0.5 * gate * gate) * (1.0 / math.sqrt(2.0 * math.pi))
    return (gate * normal_cdf, normal_cdf + gate * density)


def hidden_kernel(places, *refs):
    pieces, refs = refs[:PIECES], refs[PIECES:]
    grads, slope, value, linear, taps, linear_out, up_out, conv_out, down = refs
    peers, padded, width = grads.shape
    rows = linear_out.shape[1]
    z_count, y_count, share, half = down.shape
    first = pl.program_id(0) == 0

    @pl.when(first)
    def _():
        start = 0
        for at, piece in enumerate(pieces):
            depth = piece.shape[0]
            down[start : start + depth, pl.ds(places[at], 1)] = piece[...]
            start = (start + depth) % z_count

    per_tp = width // share
    act = jnp.zeros(slope.shape[1:], jnp.float32)
    for t in range(peers):
        z, y = divmod(t * per_tp, y_count)
        act += jnp.dot(
            grads[t],
            down[z, y : y + per_tp].reshape(width, half),
            preferred_element_type=jnp.float32,
        )
    grad = act * slope[0]

    def ahead(value, by):
        return pltpu.roll(value, padded - by, 0)

    linear_grad = (
        taps[0:1] * ahead(grad, 2) + taps[1:2] * ahead(grad, 1) + taps[2:3] * grad
    )
    linear_out[0] = linear_grad[:rows].astype(jnp.bfloat16)
    up_out[0] = ahead(act * value[0], 1)[:rows].astype(jnp.bfloat16)
    at = lax.broadcasted_iota(jnp.int32, grad.shape, 0)
    own = jnp.where((at >= 1) & (at <= rows), grad, 0.0)
    near = linear[0]
    sums = jnp.concatenate(
        [
            jnp.sum(own * (near if k == 0 else ahead(near, k)), axis=0, keepdims=True)
            for k in range(3)
        ]
    )

    @pl.when(first)
    def _():
        conv_out[...] = sums

    @pl.when(jnp.logical_not(first))
    def _():
        conv_out[...] += sums


def hidden_gradients(pieces, places, grads, slope, value, linear, taps):
    peers, padded, width = grads.shape
    z_count, _, share, half = pieces[0].shape
    y_count = peers // 2 * width // share // z_count
    rows = width
    saved = pl.BlockSpec((1, padded, half), lambda b, at: (b, 0, 0))
    made = pl.BlockSpec((1, rows, half), lambda b, at: (b, 0, 0))
    small = pl.BlockSpec((3, half), lambda b, at: (0, 0))
    return pl.pallas_call(
        hidden_kernel,
        grid_spec=pltpu.PrefetchScalarGridSpec(
            num_scalar_prefetch=1,
            grid=(2,),
            in_specs=[
                pl.BlockSpec((piece.shape[0], 1, share, half), lambda b, at: (0, 2, 0, 0))
                for piece in pieces
            ]
            + [
                pl.BlockSpec((peers // 2, padded, width), lambda b, at: (b, 0, 0)),
                saved,
                saved,
                saved,
                small,
            ],
            out_specs=[made, made, small],
            scratch_shapes=[pltpu.VMEM((z_count, y_count, share, half), jnp.bfloat16)],
        ),
        out_shape=[
            jax.ShapeDtypeStruct((2, rows, half), jnp.bfloat16),
            jax.ShapeDtypeStruct((2, rows, half), jnp.bfloat16),
            jax.ShapeDtypeStruct((3, half), jnp.float32),
        ],
    )(places, *pieces, grads, slope, value, linear, taps)


def output_kernel(places, *refs):
    pieces, (linear_grad, up_grad, out, both) = refs[:PIECES], refs[PIECES:]
    _, _, share, half = both.shape
    width = out.shape[3]
    per_tp = width // share
    z = pl.program_id(0)
    split = pl.num_programs(0) // 2

    def place(at):
        both[:, pl.ds(places[at], 1)] = pieces[at][0][:, None]

    for at in range(PIECES - 2):
        place(at)
    pl.when(z < split)(lambda: place(PIECES - 2))
    pl.when(z >= split)(lambda: place(PIECES - 1))
    contract = (((1,), (1,)), ((), ()))
    for t in range(out.shape[1]):
        gate, up = (
            both[part, t * per_tp : (t + 1) * per_tp].reshape(width, half) for part in range(2)
        )
        for b in range(2):
            part = lax.dot_general(
                linear_grad[b], gate, contract, preferred_element_type=jnp.float32
            ) + lax.dot_general(
                up_grad[b], up, contract, preferred_element_type=jnp.float32
            )
            out[b, t] = part.astype(jnp.bfloat16)


def output_partials(pieces, places, linear_grad, up_grad, width):
    _, rows, half = linear_grad.shape
    z_count, _, share, _ = pieces[0].shape
    mid = pieces[-1].shape[0]
    y_count = 8
    peers = z_count * y_count * share // width
    whole = pl.BlockSpec((2, rows, half), lambda i, at: (0, 0, 0))
    maps = [lambda i, at: (i, 0, 0, 0)] * (PIECES - 2) + [
        lambda i, at: (jnp.minimum(i, mid - 1), 0, 0, 0),
        lambda i, at: (jnp.maximum(i - mid, 0), 0, 0, 0),
    ]
    product = pl.pallas_call(
        output_kernel,
        grid_spec=pltpu.PrefetchScalarGridSpec(
            num_scalar_prefetch=1,
            grid=(z_count,),
            in_specs=[pl.BlockSpec((1, 2, share, half), m) for m in maps] + [whole, whole],
            out_specs=pl.BlockSpec((2, peers // z_count, rows, width), lambda i, at: (0, i, 0, 0)),
            scratch_shapes=[pltpu.VMEM((2, y_count, share, half), jnp.bfloat16)],
        ),
        out_shape=jax.ShapeDtypeStruct((2, peers, rows, width), jnp.bfloat16),
    )(places, *pieces, linear_grad, up_grad)
    return product.reshape(2 * peers, rows, width)


def block_gradients(out_grad, gate_lin, up_lin, conv_weight, gate_weight, up_weight, down_weight):
    rows, columns = gate_lin.shape
    width = out_grad.shape[1]
    half = columns // 2
    second = lax.axis_index("zp") == 1

    own, other = halves_of(jnp.stack([gate_weight, up_weight, down_weight.T]), second)
    pieces, places, late = gathered_y(gathered_z(own, other))

    spare = ((0, 0), (0, columns - width))
    last = jnp.concatenate([gate_lin[-2:], up_lin[-1:], jnp.pad(out_grad[-1:], spare)])
    lead = jnp.concatenate([gate_lin[:2], up_lin[:1], jnp.pad(out_grad[:1], spare)])
    before = to_next(last, SEQ_AXES, 1)
    after = to_next(lead, SEQ_AXES, -1)
    grads = jnp.concatenate(
        [
            before[3:, :width],
            out_grad,
            after[3:, :width],
            jnp.zeros((PAD - rows - 2, width), out_grad.dtype),
        ]
    )
    grads = sent_to_all(grads, GROUP)

    kept, sent = halves_of(jnp.concatenate([gate_lin, up_lin, before, after]), second)
    came = swapped(sent, "zp", 1)
    kept, came, _ = lax.optimization_barrier((kept, came, late))
    pair = jnp.stack([jnp.where(second, came, kept), jnp.where(second, kept, came)])
    pair = pair.astype(jnp.float32)
    edge = pair[:, 2 * rows :]
    linear = jnp.concatenate([edge[:, :2], pair[:, :rows], edge[:, 4:6]], axis=1)
    up_ext = jnp.concatenate([edge[:, 2:3], pair[:, rows : 2 * rows], edge[:, 6:7]], axis=1)
    start = lax.axis_index(TP) * columns + jnp.where(second, half, 0)
    taps = lax.dynamic_slice_in_dim(conv_weight, start, half, 1).astype(jnp.float32)

    gate = taps[0] * linear[:, :-2] + taps[1] * linear[:, 1:-1] + taps[2] * linear[:, 2:]
    gelu_value, gelu_slope = gelu_parts(gate)

    tail = ((0, 0), (0, PAD - rows - 2), (0, 0))
    linear_grad, up_grad, conv = hidden_gradients(
        pieces,
        places,
        grads,
        jnp.pad(up_ext * gelu_slope, tail),
        jnp.pad(gelu_value, tail),
        jnp.pad(linear, ((0, 0), (0, PAD - rows - 4), (0, 0))),
        taps,
    )
    conv = sent_to_all(conv, Z_ALL)
    conv = conv.reshape(-1, 2, 3, half).sum(axis=0).transpose(1, 0, 2).reshape(3, columns)
    product = output_partials(pieces, places, linear_grad, up_grad, width)
    arrived = lax.all_to_all(product, GROUP, 0, 0, tiled=True)
    input_grad = arrived.astype(jnp.float32).sum(axis=0).astype(jnp.bfloat16)
    for bit in (1, 2, 4):
        conv = conv + swapped(conv, "y", bit)
    conv = conv[None]
    for axis, bit in (("core", 1), ("x", 1), ("x", 2)):
        low = lax.axis_index(axis) & bit == 0
        peer = swapped(conv, axis, bit)
        conv = jnp.concatenate([jnp.where(low, conv, peer), jnp.where(low, peer, conv)])
    conv_grad = conv.transpose(1, 0, 2).reshape(3, -1)
    return (input_grad, conv_grad)


def solution(mesh):
    finer = Mesh(
        mesh.devices.reshape(mesh.shape["rep"], 2, 2, 8, 4, 2),
        ("rep", "zk", "zp", "y", "x", "core"),
    )
    return jax.shard_map(
        block_gradients,
        mesh=finer,
        in_specs=(
            P(ROWS, TP),
            P(ROWS, TP),
            P(ROWS, TP),
            P(),
            P(SEQ_AXES, TP),
            P(SEQ_AXES, TP),
            P(TP, SEQ_AXES),
        ),
        out_specs=(P(ROWS, TP), P()),
        check_vma=False,
    )
```

```python
import math

import jax
import jax.numpy as jnp
from jax import lax
from jax.experimental import pallas as pl
from jax.experimental.pallas import tpu as pltpu
from jax.sharding import Mesh
from jax.sharding import PartitionSpec as P


Z_ALL = ("rep", "zk", "zp")
SEQ_AXES = ("zk", "zp", "y")
TP = ("x", "core")
GROUP = ("zp", "x", "core")
ROWS = ("rep", "zk", "zp", "y")
PAD = 264
PIECES = 9


def shifted(value, axis, by):
    count = lax.axis_size(axis)
    return lax.ppermute(value, axis, [(i, (i + by) % count) for i in range(count)])


def to_next(value, axis, by):
    count = lax.axis_size(axis)
    pairs = [(i, i + by) for i in range(count) if 0 <= i + by < count]
    return lax.ppermute(value, axis, pairs)


def swapped(value, axis, bit):
    return lax.ppermute(value, axis, [(i, i ^ bit) for i in range(lax.axis_size(axis))])


def sent_to_all(value, axis):
    peers = lax.axis_size(axis)
    return lax.all_to_all(
        jnp.broadcast_to(value[None], (peers, *value.shape)), axis, 0, 0, tiled=True
    )


def halves_of(value, second):
    half = value.shape[-1] // 2
    left, right = value[..., :half], value[..., half:]
    return jnp.where(second, right, left), jnp.where(second, left, right)


def crossed(value, axis, by):
    names = axis if isinstance(axis, tuple) else (axis,)
    count = lax.axis_size(names)
    pairs = [
        (2 * i + core, 2 * ((i + step) % count) + core)
        for i in range(count)
        for core, step in enumerate((by, -by))
    ]
    return lax.ppermute(value, (*names, "core"), pairs)


def gathered_z(own, other):
    relative = [own, shifted(other, Z_ALL, -1), crossed(own, Z_ALL, 2), shifted(other, Z_ALL, 1)]
    count = len(relative)
    at = lax.axis_index(("zk", "zp"))
    return jnp.stack([lax.select_n((place - at) % count, *relative) for place in range(count)])


def gathered_y(block):
    mid = block.shape[0] // 2
    pieces, steps = [block], [0]
    one = two = block
    for k in range(1, 4):
        one, two = crossed(one, "y", 1), crossed(two, "y", -1)
        pieces += [one, two]
        steps += [-k, k]
    pieces += [crossed(one[:mid], "y", 1), crossed(two[mid:], "y", -1)]
    sign = 1 - 2 * lax.axis_index("core")
    count = lax.axis_size("y")
    places = (lax.axis_index("y") + sign * jnp.array(steps + [4, 4], jnp.int32)) % count
    places = jnp.append(places, lax.axis_index("core"))
    return pieces, places.astype(jnp.int32), pieces[3]


def gelu_parts(gate):
    normal_cdf = 0.5 * (1.0 + jax.scipy.special.erf(gate * (1.0 / math.sqrt(2.0))))
    density = jnp.exp(-0.5 * gate * gate) * (1.0 / math.sqrt(2.0 * math.pi))
    return (gate * normal_cdf, normal_cdf + gate * density)


def hidden_kernel(places, *refs):
    pieces, refs = refs[:PIECES], refs[PIECES:]
    grads, slope, value, linear, taps, linear_out, up_out, conv_out, down = refs
    peers, padded, width = grads.shape
    rows = linear_out.shape[1]
    z_count, y_count, share, half = down.shape
    first = pl.program_id(0) == 0

    @pl.when(first)
    def _():
        start = 0
        for at, piece in enumerate(pieces):
            depth = piece.shape[0]
            down[start : start + depth, pl.ds(places[at], 1)] = piece[...]
            start = (start + depth) % z_count

    per_tp = width // share
    act = jnp.zeros(slope.shape[1:], jnp.float32)
    for t in range(peers):
        z, y = divmod(t * per_tp, y_count)
        act += jnp.dot(
            grads[t],
            down[z, y : y + per_tp].reshape(width, half),
            preferred_element_type=jnp.float32,
        )
    grad = act * slope[0]

    def ahead(value, by):
        return pltpu.roll(value, padded - by, 0)

    linear_grad = (
        taps[0:1] * ahead(grad, 2) + taps[1:2] * ahead(grad, 1) + taps[2:3] * grad
    )
    linear_out[0] = linear_grad[:rows].astype(jnp.bfloat16)
    up_out[0] = ahead(act * value[0], 1)[:rows].astype(jnp.bfloat16)
    at = lax.broadcasted_iota(jnp.int32, grad.shape, 0)
    own = jnp.where((at >= 1) & (at <= rows), grad, 0.0)
    near = linear[0]
    sums = jnp.concatenate(
        [
            jnp.sum(own * (near if k == 0 else ahead(near, k)), axis=0, keepdims=True)
            for k in range(3)
        ]
    )

    @pl.when(first)
    def _():
        conv_out[...] = sums

    @pl.when(jnp.logical_not(first))
    def _():
        conv_out[...] += sums


def hidden_gradients(pieces, places, grads, slope, value, linear, taps):
    peers, padded, width = grads.shape
    z_count, _, share, half = pieces[0].shape
    y_count = peers // 2 * width // share // z_count
    rows = width
    saved = pl.BlockSpec((1, padded, half), lambda b, at: (b, 0, 0))
    made = pl.BlockSpec((1, rows, half), lambda b, at: (b, 0, 0))
    small = pl.BlockSpec((3, half), lambda b, at: (0, 0))
    return pl.pallas_call(
        hidden_kernel,
        grid_spec=pltpu.PrefetchScalarGridSpec(
            num_scalar_prefetch=1,
            grid=(2,),
            in_specs=[
                pl.BlockSpec((piece.shape[0], 1, share, half), lambda b, at: (0, 2, 0, 0))
                for piece in pieces
            ]
            + [
                pl.BlockSpec((peers // 2, padded, width), lambda b, at: (b, 0, 0)),
                saved,
                saved,
                saved,
                small,
            ],
            out_specs=[made, made, small],
            scratch_shapes=[pltpu.VMEM((z_count, y_count, share, half), jnp.bfloat16)],
        ),
        out_shape=[
            jax.ShapeDtypeStruct((2, rows, half), jnp.bfloat16),
            jax.ShapeDtypeStruct((2, rows, half), jnp.bfloat16),
            jax.ShapeDtypeStruct((3, half), jnp.float32),
        ],
    )(places, *pieces, grads, slope, value, linear, taps)


def output_kernel(places, *refs):
    pieces, (linear_grad, up_grad, kept, sent, both) = refs[:PIECES], refs[PIECES:]
    _, _, share, half = both.shape
    width = kept.shape[3]
    per_tp = width // share
    z = pl.program_id(0)
    split = pl.num_programs(0) // 2

    def place(at):
        both[:, pl.ds(places[at], 1)] = pieces[at][0][:, None]

    for at in range(PIECES - 2):
        place(at)
    pl.when(z < split)(lambda: place(PIECES - 2))
    pl.when(z >= split)(lambda: place(PIECES - 1))
    contract = (((1,), (1,)), ((), ()))
    core = places[PIECES]
    for target, out in ((core, kept), (1 - core, sent)):
        gate, up = (
            both[part, pl.ds(target * per_tp, per_tp)].reshape(width, half) for part in range(2)
        )
        for b in range(2):
            part = lax.dot_general(
                linear_grad[b], gate, contract, preferred_element_type=jnp.float32
            ) + lax.dot_general(
                up_grad[b], up, contract, preferred_element_type=jnp.float32
            )
            out[b, 0] = part.astype(jnp.bfloat16)


def output_partials(pieces, places, linear_grad, up_grad, width):
    _, rows, half = linear_grad.shape
    z_count, _, share, _ = pieces[0].shape
    mid = pieces[-1].shape[0]
    y_count = 2 * width // share
    whole = pl.BlockSpec((2, rows, half), lambda i, at: (0, 0, 0))
    maps = [lambda i, at: (i, 0, 0, 0)] * (PIECES - 2) + [
        lambda i, at: (jnp.minimum(i, mid - 1), 0, 0, 0),
        lambda i, at: (jnp.maximum(i - mid, 0), 0, 0, 0),
    ]
    made = pl.BlockSpec((2, 1, rows, width), lambda i, at: (0, i, 0, 0))
    shape = jax.ShapeDtypeStruct((2, z_count, rows, width), jnp.bfloat16)
    return pl.pallas_call(
        output_kernel,
        grid_spec=pltpu.PrefetchScalarGridSpec(
            num_scalar_prefetch=1,
            grid=(z_count,),
            in_specs=[pl.BlockSpec((1, 2, share, half), m) for m in maps] + [whole, whole],
            out_specs=[made, made],
            scratch_shapes=[pltpu.VMEM((2, y_count, share, half), jnp.bfloat16)],
        ),
        out_shape=[shape, shape],
    )(places, *pieces, linear_grad, up_grad)


def block_gradients(out_grad, gate_lin, up_lin, conv_weight, gate_weight, up_weight, down_weight):
    rows, columns = gate_lin.shape
    width = out_grad.shape[1]
    half = columns // 2
    second = lax.axis_index("zp") == 1

    own, other = halves_of(jnp.stack([gate_weight, up_weight, down_weight.T]), second)
    pieces, places, late = gathered_y(gathered_z(own, other))

    spare = ((0, 0), (0, columns - width))
    last = jnp.concatenate([gate_lin[-2:], up_lin[-1:], jnp.pad(out_grad[-1:], spare)])
    lead = jnp.concatenate([gate_lin[:2], up_lin[:1], jnp.pad(out_grad[:1], spare)])
    before = to_next(last, SEQ_AXES, 1)
    after = to_next(lead, SEQ_AXES, -1)
    grads = jnp.concatenate(
        [
            before[3:, :width],
            out_grad,
            after[3:, :width],
            jnp.zeros((PAD - rows - 2, width), out_grad.dtype),
        ]
    )
    grads = sent_to_all(grads, GROUP)

    kept, sent = halves_of(jnp.concatenate([gate_lin, up_lin, before, after]), second)
    came = swapped(sent, "zp", 1)
    kept, came, _ = lax.optimization_barrier((kept, came, late))
    pair = jnp.stack([jnp.where(second, came, kept), jnp.where(second, kept, came)])
    pair = pair.astype(jnp.float32)
    edge = pair[:, 2 * rows :]
    linear = jnp.concatenate([edge[:, :2], pair[:, :rows], edge[:, 4:6]], axis=1)
    up_ext = jnp.concatenate([edge[:, 2:3], pair[:, rows : 2 * rows], edge[:, 6:7]], axis=1)
    start = lax.axis_index(TP) * columns + jnp.where(second, half, 0)
    taps = lax.dynamic_slice_in_dim(conv_weight, start, half, 1).astype(jnp.float32)

    gate = taps[0] * linear[:, :-2] + taps[1] * linear[:, 1:-1] + taps[2] * linear[:, 2:]
    gelu_value, gelu_slope = gelu_parts(gate)

    tail = ((0, 0), (0, PAD - rows - 2), (0, 0))
    linear_grad, up_grad, conv = hidden_gradients(
        pieces,
        places,
        grads,
        jnp.pad(up_ext * gelu_slope, tail),
        jnp.pad(gelu_value, tail),
        jnp.pad(linear, ((0, 0), (0, PAD - rows - 4), (0, 0))),
        taps,
    )
    conv = sent_to_all(conv, Z_ALL)
    conv = conv.reshape(-1, 2, 3, half).sum(axis=0).transpose(1, 0, 2).reshape(3, columns)
    kept, sent = output_partials(pieces, places, linear_grad, up_grad, width)
    came = swapped(sent, "core", 1)
    product = (kept.astype(jnp.float32) + came.astype(jnp.float32)).astype(jnp.bfloat16)
    conv = sent_to_all(conv, "y")
    conv = conv.sum(axis=0)
    arrived = lax.all_to_all(
        product.reshape(-1, rows, width), ("zp", "x"), 0, 0, tiled=True
    )
    input_grad = arrived.astype(jnp.float32).sum(axis=0).astype(jnp.bfloat16)
    conv = conv[None]
    for axis, bit in (("core", 1), ("x", 1), ("x", 2)):
        low = lax.axis_index(axis) & bit == 0
        peer = swapped(conv, axis, bit)
        conv = jnp.concatenate([jnp.where(low, conv, peer), jnp.where(low, peer, conv)])
    conv_grad = conv.transpose(1, 0, 2).reshape(3, -1)
    return (input_grad, conv_grad)


def solution(mesh):
    finer = Mesh(
        mesh.devices.reshape(mesh.shape["rep"], 2, 2, 8, 4, 2),
        ("rep", "zk", "zp", "y", "x", "core"),
    )
    return jax.shard_map(
        block_gradients,
        mesh=finer,
        in_specs=(
            P(ROWS, TP),
            P(ROWS, TP),
            P(ROWS, TP),
            P(),
            P(SEQ_AXES, TP),
            P(SEQ_AXES, TP),
            P(TP, SEQ_AXES),
        ),
        out_specs=(P(ROWS, TP), P()),
        check_vma=False,
    )
```

```python
import math

import jax
import jax.numpy as jnp
from jax import lax
from jax.experimental import pallas as pl
from jax.experimental.pallas import tpu as pltpu
from jax.sharding import Mesh
from jax.sharding import PartitionSpec as P


Z_ALL = ("rep", "zk", "zp")
SEQ_AXES = ("zk", "zp", "y")
TP = ("x", "core")
GROUP = ("zp", "x", "core")
ROWS = ("rep", "zk", "zp", "y")
PAD = 264
PIECES = 9


def shifted(value, axis, by):
    count = lax.axis_size(axis)
    return lax.ppermute(value, axis, [(i, (i + by) % count) for i in range(count)])


def to_next(value, axis, by):
    count = lax.axis_size(axis)
    pairs = [(i, i + by) for i in range(count) if 0 <= i + by < count]
    return lax.ppermute(value, axis, pairs)


def swapped(value, axis, bit):
    return lax.ppermute(value, axis, [(i, i ^ bit) for i in range(lax.axis_size(axis))])


def sent_to_all(value, axis):
    peers = lax.axis_size(axis)
    return lax.all_to_all(
        jnp.broadcast_to(value[None], (peers, *value.shape)), axis, 0, 0, tiled=True
    )


def halves_of(value, second):
    half = value.shape[-1] // 2
    left, right = value[..., :half], value[..., half:]
    return jnp.where(second, right, left), jnp.where(second, left, right)


def crossed(value, axis, by):
    names = axis if isinstance(axis, tuple) else (axis,)
    count = lax.axis_size(names)
    pairs = [
        (2 * i + core, 2 * ((i + step) % count) + core)
        for i in range(count)
        for core, step in enumerate((by, -by))
    ]
    return lax.ppermute(value, (*names, "core"), pairs)


def gathered_z(own, other):
    relative = [own, shifted(other, Z_ALL, -1), crossed(own, Z_ALL, 2), shifted(other, Z_ALL, 1)]
    count = len(relative)
    at = lax.axis_index(("zk", "zp"))
    return jnp.stack([lax.select_n((place - at) % count, *relative) for place in range(count)])


def gathered_y(block):
    mid = block.shape[0] // 2
    pieces, steps = [block], [0]
    one = two = block
    for k in range(1, 4):
        one, two = shifted(one, "y", 1), shifted(two, "y", -1)
        pieces += [one, two]
        steps += [-k, k]
    pieces += [shifted(one[:mid], "y", 1), shifted(two[mid:], "y", -1)]
    count = lax.axis_size("y")
    places = (lax.axis_index("y") + jnp.array(steps + [4, 4], jnp.int32)) % count
    places = jnp.append(places, lax.axis_index("core"))
    return pieces, places.astype(jnp.int32), pieces[3]


def gelu_parts(gate):
    normal_cdf = 0.5 * (1.0 + jax.scipy.special.erf(gate * (1.0 / math.sqrt(2.0))))
    density = jnp.exp(-0.5 * gate * gate) * (1.0 / math.sqrt(2.0 * math.pi))
    return (gate * normal_cdf, normal_cdf + gate * density)


def hidden_kernel(places, *refs):
    pieces, refs = refs[:PIECES], refs[PIECES:]
    grads, slope, value, linear, taps, linear_out, up_out, conv_out, down = refs
    peers, padded, width = grads.shape
    rows = linear_out.shape[1]
    z_count, y_count, share, half = down.shape
    first = pl.program_id(0) == 0

    @pl.when(first)
    def _():
        start = 0
        for at, piece in enumerate(pieces):
            depth = piece.shape[0]
            down[start : start + depth, pl.ds(places[at], 1)] = piece[...]
            start = (start + depth) % z_count

    per_tp = width // share
    act = jnp.zeros(slope.shape[1:], jnp.float32)
    for t in range(peers):
        z, y = divmod(t * per_tp, y_count)
        act += jnp.dot(
            grads[t],
            down[z, y : y + per_tp].reshape(width, half),
            preferred_element_type=jnp.float32,
        )
    grad = act * slope[0]

    def ahead(value, by):
        return pltpu.roll(value, padded - by, 0)

    linear_grad = (
        taps[0:1] * ahead(grad, 2) + taps[1:2] * ahead(grad, 1) + taps[2:3] * grad
    )
    linear_out[0] = linear_grad[:rows].astype(jnp.bfloat16)
    up_out[0] = ahead(act * value[0], 1)[:rows].astype(jnp.bfloat16)
    at = lax.broadcasted_iota(jnp.int32, grad.shape, 0)
    own = jnp.where((at >= 1) & (at <= rows), grad, 0.0)
    near = linear[0]
    sums = jnp.concatenate(
        [
            jnp.sum(own * (near if k == 0 else ahead(near, k)), axis=0, keepdims=True)
            for k in range(3)
        ]
    )

    @pl.when(first)
    def _():
        conv_out[...] = sums

    @pl.when(jnp.logical_not(first))
    def _():
        conv_out[...] += sums


def hidden_gradients(pieces, places, grads, slope, value, linear, taps):
    peers, padded, width = grads.shape
    z_count, _, share, half = pieces[0].shape
    y_count = peers // 2 * width // share // z_count
    rows = width
    saved = pl.BlockSpec((1, padded, half), lambda b, at: (b, 0, 0))
    made = pl.BlockSpec((1, rows, half), lambda b, at: (b, 0, 0))
    small = pl.BlockSpec((3, half), lambda b, at: (0, 0))
    return pl.pallas_call(
        hidden_kernel,
        grid_spec=pltpu.PrefetchScalarGridSpec(
            num_scalar_prefetch=1,
            grid=(2,),
            in_specs=[
                pl.BlockSpec((piece.shape[0], 1, share, half), lambda b, at: (0, 2, 0, 0))
                for piece in pieces
            ]
            + [
                pl.BlockSpec((peers // 2, padded, width), lambda b, at: (b, 0, 0)),
                saved,
                saved,
                saved,
                small,
            ],
            out_specs=[made, made, small],
            scratch_shapes=[pltpu.VMEM((z_count, y_count, share, half), jnp.bfloat16)],
        ),
        out_shape=[
            jax.ShapeDtypeStruct((2, rows, half), jnp.bfloat16),
            jax.ShapeDtypeStruct((2, rows, half), jnp.bfloat16),
            jax.ShapeDtypeStruct((3, half), jnp.float32),
        ],
    )(places, *pieces, grads, slope, value, linear, taps)


def output_kernel(places, *refs):
    pieces, (linear_grad, up_grad, kept, sent, both) = refs[:PIECES], refs[PIECES:]
    _, _, share, half = both.shape
    width = kept.shape[3]
    per_tp = width // share
    z = pl.program_id(0)
    split = pl.num_programs(0) // 2

    def place(at):
        both[:, pl.ds(places[at], 1)] = pieces[at][0][:, None]

    for at in range(PIECES - 2):
        place(at)
    pl.when(z < split)(lambda: place(PIECES - 2))
    pl.when(z >= split)(lambda: place(PIECES - 1))
    contract = (((1,), (1,)), ((), ()))
    core = places[PIECES]
    for target, out in ((core, kept), (1 - core, sent)):
        gate, up = (
            both[part, pl.ds(target * per_tp, per_tp)].reshape(width, half) for part in range(2)
        )
        for b in range(2):
            part = lax.dot_general(
                linear_grad[b], gate, contract, preferred_element_type=jnp.float32
            ) + lax.dot_general(
                up_grad[b], up, contract, preferred_element_type=jnp.float32
            )
            out[b, 0] = part.astype(jnp.bfloat16)


def output_partials(pieces, places, linear_grad, up_grad, width):
    _, rows, half = linear_grad.shape
    z_count, _, share, _ = pieces[0].shape
    mid = pieces[-1].shape[0]
    y_count = 2 * width // share
    whole = pl.BlockSpec((2, rows, half), lambda i, at: (0, 0, 0))
    maps = [lambda i, at: (i, 0, 0, 0)] * (PIECES - 2) + [
        lambda i, at: (jnp.minimum(i, mid - 1), 0, 0, 0),
        lambda i, at: (jnp.maximum(i - mid, 0), 0, 0, 0),
    ]
    made = pl.BlockSpec((2, 1, rows, width), lambda i, at: (0, i, 0, 0))
    shape = jax.ShapeDtypeStruct((2, z_count, rows, width), jnp.bfloat16)
    return pl.pallas_call(
        output_kernel,
        grid_spec=pltpu.PrefetchScalarGridSpec(
            num_scalar_prefetch=1,
            grid=(z_count,),
            in_specs=[pl.BlockSpec((1, 2, share, half), m) for m in maps] + [whole, whole],
            out_specs=[made, made],
            scratch_shapes=[pltpu.VMEM((2, y_count, share, half), jnp.bfloat16)],
        ),
        out_shape=[shape, shape],
    )(places, *pieces, linear_grad, up_grad)


def block_gradients(out_grad, gate_lin, up_lin, conv_weight, gate_weight, up_weight, down_weight):
    rows, columns = gate_lin.shape
    width = out_grad.shape[1]
    half = columns // 2
    second = lax.axis_index("zp") == 1

    own, other = halves_of(jnp.stack([gate_weight, up_weight, down_weight.T]), second)
    pieces, places, late = gathered_y(gathered_z(own, other))

    spare = ((0, 0), (0, columns - width))
    last = jnp.concatenate([gate_lin[-2:], up_lin[-1:], jnp.pad(out_grad[-1:], spare)])
    lead = jnp.concatenate([gate_lin[:2], up_lin[:1], jnp.pad(out_grad[:1], spare)])
    before = to_next(last, SEQ_AXES, 1)
    after = to_next(lead, SEQ_AXES, -1)
    grads = jnp.concatenate(
        [
            before[3:, :width],
            out_grad,
            after[3:, :width],
            jnp.zeros((PAD - rows - 2, width), out_grad.dtype),
        ]
    )
    grads = sent_to_all(grads, GROUP)

    kept, sent = halves_of(jnp.concatenate([gate_lin, up_lin, before, after]), second)
    came = swapped(sent, "zp", 1)
    kept, came, _ = lax.optimization_barrier((kept, came, late))
    pair = jnp.stack([jnp.where(second, came, kept), jnp.where(second, kept, came)])
    pair = pair.astype(jnp.float32)
    edge = pair[:, 2 * rows :]
    linear = jnp.concatenate([edge[:, :2], pair[:, :rows], edge[:, 4:6]], axis=1)
    up_ext = jnp.concatenate([edge[:, 2:3], pair[:, rows : 2 * rows], edge[:, 6:7]], axis=1)
    start = lax.axis_index(TP) * columns + jnp.where(second, half, 0)
    taps = lax.dynamic_slice_in_dim(conv_weight, start, half, 1).astype(jnp.float32)

    gate = taps[0] * linear[:, :-2] + taps[1] * linear[:, 1:-1] + taps[2] * linear[:, 2:]
    gelu_value, gelu_slope = gelu_parts(gate)

    tail = ((0, 0), (0, PAD - rows - 2), (0, 0))
    linear_grad, up_grad, conv = hidden_gradients(
        pieces,
        places,
        grads,
        jnp.pad(up_ext * gelu_slope, tail),
        jnp.pad(gelu_value, tail),
        jnp.pad(linear, ((0, 0), (0, PAD - rows - 4), (0, 0))),
        taps,
    )
    conv = sent_to_all(conv, Z_ALL)
    conv = conv.reshape(-1, 2, 3, half).sum(axis=0).transpose(1, 0, 2).reshape(3, columns)
    kept, sent = output_partials(pieces, places, linear_grad, up_grad, width)
    came = swapped(sent, "core", 1)
    product = (kept.astype(jnp.float32) + came.astype(jnp.float32)).astype(jnp.bfloat16)
    conv = sent_to_all(conv, "y")
    conv = conv.sum(axis=0)
    arrived = lax.all_to_all(
        product.reshape(-1, rows, width), ("zp", "x"), 0, 0, tiled=True
    )
    input_grad = arrived.astype(jnp.float32).sum(axis=0).astype(jnp.bfloat16)
    conv = lax.all_gather(conv, TP)
    conv_grad = conv.transpose(1, 0, 2).reshape(3, -1)
    return (input_grad, conv_grad)


def solution(mesh):
    finer = Mesh(
        mesh.devices.reshape(mesh.shape["rep"], 2, 2, 8, 4, 2),
        ("rep", "zk", "zp", "y", "x", "core"),
    )
    return jax.shard_map(
        block_gradients,
        mesh=finer,
        in_specs=(
            P(ROWS, TP),
            P(ROWS, TP),
            P(ROWS, TP),
            P(),
            P(SEQ_AXES, TP),
            P(SEQ_AXES, TP),
            P(TP, SEQ_AXES),
        ),
        out_specs=(P(ROWS, TP), P()),
        check_vma=False,
    )
```

```python
import math

import jax
import jax.numpy as jnp
from jax import lax
from jax.experimental import pallas as pl
from jax.experimental.pallas import tpu as pltpu
from jax.sharding import Mesh
from jax.sharding import PartitionSpec as P


Z_ALL = ("rep", "zk", "zp")
SEQ_AXES = ("zk", "zp", "y")
TP = ("x", "core")
ROWS = ("rep", "zk", "zp", "y")
PAD = 264
PIECES = 9


def shifted(value, axis, by):
    count = lax.axis_size(axis)
    return lax.ppermute(value, axis, [(i, (i + by) % count) for i in range(count)])


def to_next(value, axis, by):
    count = lax.axis_size(axis)
    pairs = [(i, i + by) for i in range(count) if 0 <= i + by < count]
    return lax.ppermute(value, axis, pairs)


def swapped(value, axis, bit):
    return lax.ppermute(value, axis, [(i, i ^ bit) for i in range(lax.axis_size(axis))])


def sent_to_all(value, axis):
    peers = lax.axis_size(axis)
    return lax.all_to_all(
        jnp.broadcast_to(value[None], (peers, *value.shape)), axis, 0, 0, tiled=True
    )


def halves_of(value, second):
    half = value.shape[-1] // 2
    left, right = value[..., :half], value[..., half:]
    return jnp.where(second, right, left), jnp.where(second, left, right)


def crossed(value, axis, by):
    names = axis if isinstance(axis, tuple) else (axis,)
    count = lax.axis_size(names)
    pairs = [
        (2 * i + core, 2 * ((i + step) % count) + core)
        for i in range(count)
        for core, step in enumerate((by, -by))
    ]
    return lax.ppermute(value, (*names, "core"), pairs)


def gathered_z(own, other):
    relative = [own, shifted(other, Z_ALL, -1), crossed(own, Z_ALL, 2), shifted(other, Z_ALL, 1)]
    count = len(relative)
    at = lax.axis_index(("zk", "zp"))
    return jnp.stack([lax.select_n((place - at) % count, *relative) for place in range(count)])


def gathered_y(block):
    mid = block.shape[0] // 2
    pieces, steps = [block], [0]
    one = two = block
    for k in range(1, 4):
        one, two = shifted(one, "y", 1), shifted(two, "y", -1)
        pieces += [one, two]
        steps += [-k, k]
    pieces += [shifted(one[:mid], "y", 1), shifted(two[mid:], "y", -1)]
    count = lax.axis_size("y")
    places = (lax.axis_index("y") + jnp.array(steps + [4, 4], jnp.int32)) % count
    places = jnp.append(places, lax.axis_index("core"))
    return pieces, places.astype(jnp.int32), pieces[3]


def gelu_parts(gate):
    normal_cdf = 0.5 * (1.0 + jax.scipy.special.erf(gate * (1.0 / math.sqrt(2.0))))
    density = jnp.exp(-0.5 * gate * gate) * (1.0 / math.sqrt(2.0 * math.pi))
    return (gate * normal_cdf, normal_cdf + gate * density)


def hidden_kernel(places, *refs):
    pieces, refs = refs[:PIECES], refs[PIECES:]
    grads, shared, slope, value, linear, taps, linear_out, up_out, conv_out, down = refs
    _, padded, width = grads.shape
    rows = linear_out.shape[1]
    z_count, _, share, half = down.shape
    first = pl.program_id(0) == 0

    @pl.when(first)
    def _():
        start = 0
        for at, piece in enumerate(pieces):
            depth = piece.shape[0]
            down[start : start + depth, pl.ds(places[at], 1)] = piece[...]
            start = (start + depth) % z_count

    per_tp = width // share
    act = jnp.zeros(slope.shape[1:], jnp.float32)
    core = places[PIECES]
    for z in range(z_count):
        for part, owner in ((grads, core), (shared, 1 - core)):
            act += jnp.dot(
                part[z],
                down[z, pl.ds(owner * per_tp, per_tp)].reshape(width, half),
                preferred_element_type=jnp.float32,
            )
    grad = act * slope[0]

    def ahead(value, by):
        return pltpu.roll(value, padded - by, 0)

    linear_grad = (
        taps[0:1] * ahead(grad, 2) + taps[1:2] * ahead(grad, 1) + taps[2:3] * grad
    )
    linear_out[0] = linear_grad[:rows].astype(jnp.bfloat16)
    up_out[0] = ahead(act * value[0], 1)[:rows].astype(jnp.bfloat16)
    at = lax.broadcasted_iota(jnp.int32, grad.shape, 0)
    own = jnp.where((at >= 1) & (at <= rows), grad, 0.0)
    near = linear[0]
    sums = jnp.concatenate(
        [
            jnp.sum(own * (near if k == 0 else ahead(near, k)), axis=0, keepdims=True)
            for k in range(3)
        ]
    )

    @pl.when(first)
    def _():
        conv_out[...] = sums

    @pl.when(jnp.logical_not(first))
    def _():
        conv_out[...] += sums


def hidden_gradients(pieces, places, grads, shared, slope, value, linear, taps):
    peers, padded, width = grads.shape
    z_count, _, share, half = pieces[0].shape
    y_count = 2 * width // share
    rows = width
    saved = pl.BlockSpec((1, padded, half), lambda b, at: (b, 0, 0))
    made = pl.BlockSpec((1, rows, half), lambda b, at: (b, 0, 0))
    small = pl.BlockSpec((3, half), lambda b, at: (0, 0))
    return pl.pallas_call(
        hidden_kernel,
        grid_spec=pltpu.PrefetchScalarGridSpec(
            num_scalar_prefetch=1,
            grid=(2,),
            in_specs=[
                pl.BlockSpec((piece.shape[0], 1, share, half), lambda b, at: (0, 2, 0, 0))
                for piece in pieces
            ]
            + [
                pl.BlockSpec((peers // 2, padded, width), lambda b, at: (b, 0, 0)),
                pl.BlockSpec((peers // 2, padded, width), lambda b, at: (b, 0, 0)),
                saved,
                saved,
                saved,
                small,
            ],
            out_specs=[made, made, small],
            scratch_shapes=[pltpu.VMEM((z_count, y_count, share, half), jnp.bfloat16)],
        ),
        out_shape=[
            jax.ShapeDtypeStruct((2, rows, half), jnp.bfloat16),
            jax.ShapeDtypeStruct((2, rows, half), jnp.bfloat16),
            jax.ShapeDtypeStruct((3, half), jnp.float32),
        ],
    )(places, *pieces, grads, shared, slope, value, linear, taps)


def output_kernel(places, *refs):
    pieces, (linear_grad, up_grad, kept, sent, both) = refs[:PIECES], refs[PIECES:]
    _, _, share, half = both.shape
    width = kept.shape[3]
    per_tp = width // share
    z = pl.program_id(0)
    split = pl.num_programs(0) // 2

    def place(at):
        both[:, pl.ds(places[at], 1)] = pieces[at][0][:, None]

    for at in range(PIECES - 2):
        place(at)
    pl.when(z < split)(lambda: place(PIECES - 2))
    pl.when(z >= split)(lambda: place(PIECES - 1))
    contract = (((1,), (1,)), ((), ()))
    core = places[PIECES]
    for target, out in ((core, kept), (1 - core, sent)):
        gate, up = (
            both[part, pl.ds(target * per_tp, per_tp)].reshape(width, half) for part in range(2)
        )
        for b in range(2):
            part = lax.dot_general(
                linear_grad[b], gate, contract, preferred_element_type=jnp.float32
            ) + lax.dot_general(
                up_grad[b], up, contract, preferred_element_type=jnp.float32
            )
            out[b, 0] = part.astype(jnp.bfloat16)


def output_partials(pieces, places, linear_grad, up_grad, width):
    _, rows, half = linear_grad.shape
    z_count, _, share, _ = pieces[0].shape
    mid = pieces[-1].shape[0]
    y_count = 2 * width // share
    whole = pl.BlockSpec((2, rows, half), lambda i, at: (0, 0, 0))
    maps = [lambda i, at: (i, 0, 0, 0)] * (PIECES - 2) + [
        lambda i, at: (jnp.minimum(i, mid - 1), 0, 0, 0),
        lambda i, at: (jnp.maximum(i - mid, 0), 0, 0, 0),
    ]
    made = pl.BlockSpec((2, 1, rows, width), lambda i, at: (0, i, 0, 0))
    shape = jax.ShapeDtypeStruct((2, z_count, rows, width), jnp.bfloat16)
    return pl.pallas_call(
        output_kernel,
        grid_spec=pltpu.PrefetchScalarGridSpec(
            num_scalar_prefetch=1,
            grid=(z_count,),
            in_specs=[pl.BlockSpec((1, 2, share, half), m) for m in maps] + [whole, whole],
            out_specs=[made, made],
            scratch_shapes=[pltpu.VMEM((2, y_count, share, half), jnp.bfloat16)],
        ),
        out_shape=[shape, shape],
    )(places, *pieces, linear_grad, up_grad)


def block_gradients(out_grad, gate_lin, up_lin, conv_weight, gate_weight, up_weight, down_weight):
    rows, columns = gate_lin.shape
    width = out_grad.shape[1]
    half = columns // 2
    second = lax.axis_index("zp") == 1

    own, other = halves_of(jnp.stack([gate_weight, up_weight, down_weight.T]), second)
    pieces, places, late = gathered_y(gathered_z(own, other))

    spare = ((0, 0), (0, columns - width))
    last = jnp.concatenate([gate_lin[-2:], up_lin[-1:], jnp.pad(out_grad[-1:], spare)])
    lead = jnp.concatenate([gate_lin[:2], up_lin[:1], jnp.pad(out_grad[:1], spare)])
    before = to_next(last, SEQ_AXES, 1)
    after = to_next(lead, SEQ_AXES, -1)
    grads = jnp.concatenate(
        [
            before[3:, :width],
            out_grad,
            after[3:, :width],
            jnp.zeros((PAD - rows - 2, width), out_grad.dtype),
        ]
    )
    grads = sent_to_all(grads, ("zp", "x"))
    shared = swapped(grads, "core", 1)

    kept, sent = halves_of(jnp.concatenate([gate_lin, up_lin, before, after]), second)
    came = swapped(sent, "zp", 1)
    kept, came, _ = lax.optimization_barrier((kept, came, late))
    pair = jnp.stack([jnp.where(second, came, kept), jnp.where(second, kept, came)])
    pair = pair.astype(jnp.float32)
    edge = pair[:, 2 * rows :]
    linear = jnp.concatenate([edge[:, :2], pair[:, :rows], edge[:, 4:6]], axis=1)
    up_ext = jnp.concatenate([edge[:, 2:3], pair[:, rows : 2 * rows], edge[:, 6:7]], axis=1)
    start = lax.axis_index(TP) * columns + jnp.where(second, half, 0)
    taps = lax.dynamic_slice_in_dim(conv_weight, start, half, 1).astype(jnp.float32)

    gate = taps[0] * linear[:, :-2] + taps[1] * linear[:, 1:-1] + taps[2] * linear[:, 2:]
    gelu_value, gelu_slope = gelu_parts(gate)

    tail = ((0, 0), (0, PAD - rows - 2), (0, 0))
    linear_grad, up_grad, conv = hidden_gradients(
        pieces,
        places,
        grads,
        shared,
        jnp.pad(up_ext * gelu_slope, tail),
        jnp.pad(gelu_value, tail),
        jnp.pad(linear, ((0, 0), (0, PAD - rows - 4), (0, 0))),
        taps,
    )
    conv = sent_to_all(conv, Z_ALL)
    conv = conv.reshape(-1, 2, 3, half).sum(axis=0).transpose(1, 0, 2).reshape(3, columns)
    kept, sent = output_partials(pieces, places, linear_grad, up_grad, width)
    came = swapped(sent, "core", 1)
    product = (kept.astype(jnp.float32) + came.astype(jnp.float32)).astype(jnp.bfloat16)
    conv = sent_to_all(conv, "y")
    conv = conv.sum(axis=0)
    arrived = lax.all_to_all(
        product.reshape(-1, rows, width), ("zp", "x"), 0, 0, tiled=True
    )
    input_grad = arrived.astype(jnp.float32).sum(axis=0).astype(jnp.bfloat16)
    conv = lax.all_gather(conv, TP)
    conv_grad = conv.transpose(1, 0, 2).reshape(3, -1)
    return (input_grad, conv_grad)


def solution(mesh):
    finer = Mesh(
        mesh.devices.reshape(mesh.shape["rep"], 2, 2, 8, 4, 2),
        ("rep", "zk", "zp", "y", "x", "core"),
    )
    return jax.shard_map(
        block_gradients,
        mesh=finer,
        in_specs=(
            P(ROWS, TP),
            P(ROWS, TP),
            P(ROWS, TP),
            P(),
            P(SEQ_AXES, TP),
            P(SEQ_AXES, TP),
            P(TP, SEQ_AXES),
        ),
        out_specs=(P(ROWS, TP), P()),
        check_vma=False,
    )
```

```python
import math

import jax
import jax.numpy as jnp
from jax import lax
from jax.experimental import pallas as pl
from jax.experimental.pallas import tpu as pltpu
from jax.sharding import Mesh
from jax.sharding import PartitionSpec as P


Z_ALL = ("rep", "zk", "zp")
SEQ_AXES = ("zk", "zp", "y")
TP = ("x", "core")
ROWS = ("rep", "zk", "zp", "y")
PAD = 264
PIECES = 9


def shifted(value, axis, by):
    count = lax.axis_size(axis)
    return lax.ppermute(value, axis, [(i, (i + by) % count) for i in range(count)])


def to_next(value, axis, by):
    count = lax.axis_size(axis)
    pairs = [(i, i + by) for i in range(count) if 0 <= i + by < count]
    return lax.ppermute(value, axis, pairs)


def swapped(value, axis, bit):
    return lax.ppermute(value, axis, [(i, i ^ bit) for i in range(lax.axis_size(axis))])


def sent_to_all(value, axis):
    peers = lax.axis_size(axis)
    return lax.all_to_all(
        jnp.broadcast_to(value[None], (peers, *value.shape)), axis, 0, 0, tiled=True
    )


def halves_of(value, second):
    half = value.shape[-1] // 2
    left, right = value[..., :half], value[..., half:]
    return jnp.where(second, right, left), jnp.where(second, left, right)


def crossed(value, axis, by):
    names = axis if isinstance(axis, tuple) else (axis,)
    count = lax.axis_size(names)
    pairs = [
        (2 * i + core, 2 * ((i + step) % count) + core)
        for i in range(count)
        for core, step in enumerate((by, -by))
    ]
    return lax.ppermute(value, (*names, "core"), pairs)


def gathered_z(own, other):
    relative = [own, shifted(other, Z_ALL, -1), crossed(own, Z_ALL, 2), shifted(other, Z_ALL, 1)]
    count = len(relative)
    at = lax.axis_index(("zk", "zp"))
    return jnp.stack([lax.select_n((place - at) % count, *relative) for place in range(count)])


def gathered_y(block):
    mid = block.shape[0] // 2
    pieces, steps = [block], [0]
    one = two = block
    for k in range(1, 4):
        one, two = shifted(one, "y", 1), shifted(two, "y", -1)
        pieces += [one, two]
        steps += [-k, k]
    pieces += [shifted(one[:mid], "y", 1), shifted(two[mid:], "y", -1)]
    count = lax.axis_size("y")
    places = (lax.axis_index("y") + jnp.array(steps + [4, 4], jnp.int32)) % count
    places = jnp.append(places, lax.axis_index("core"))
    return pieces, places.astype(jnp.int32), pieces[3]


def gelu_parts(gate):
    normal_cdf = 0.5 * (1.0 + jax.scipy.special.erf(gate * (1.0 / math.sqrt(2.0))))
    density = jnp.exp(-0.5 * gate * gate) * (1.0 / math.sqrt(2.0 * math.pi))
    return (gate * normal_cdf, normal_cdf + gate * density)


def hidden_kernel(places, *refs):
    pieces, refs = refs[:PIECES], refs[PIECES:]
    grads, shared, slope, value, linear, taps, linear_out, up_out, conv_out, down, total = refs
    _, padded, width = grads.shape
    rows = linear_out.shape[1]
    z_count, _, share, half = down.shape
    first = pl.program_id(0) == 0

    @pl.when(first)
    def _():
        start = 0
        for at, piece in enumerate(pieces):
            depth = piece.shape[0]
            down[start : start + depth, pl.ds(places[at], 1)] = piece[...]
            start = (start + depth) % z_count

    per_tp = width // share
    act = jnp.zeros(slope.shape[1:], jnp.float32)
    core = places[PIECES]
    for z in range(z_count):
        for part, owner in ((grads, core), (shared, 1 - core)):
            act += jnp.dot(
                part[z],
                down[z, pl.ds(owner * per_tp, per_tp)].reshape(width, half),
                preferred_element_type=jnp.float32,
            )
    grad = act * slope[0]

    def ahead(value, by):
        return pltpu.roll(value, padded - by, 0)

    linear_grad = (
        taps[0:1] * ahead(grad, 2) + taps[1:2] * ahead(grad, 1) + taps[2:3] * grad
    )
    linear_out[0] = linear_grad[:rows].astype(jnp.bfloat16)
    up_out[0] = ahead(act * value[0], 1)[:rows].astype(jnp.bfloat16)
    at = lax.broadcasted_iota(jnp.int32, grad.shape, 0)
    own = jnp.where((at >= 1) & (at <= rows), grad, 0.0)
    near = linear[0]
    sums = jnp.concatenate(
        [
            jnp.sum(own * (near if k == 0 else ahead(near, k)), axis=0, keepdims=True)
            for k in range(3)
        ]
    )

    @pl.when(first)
    def _():
        total[...] = sums

    @pl.when(jnp.logical_not(first))
    def _():
        conv_out[...] = jnp.broadcast_to((total[...] + sums)[None], conv_out.shape)


def hidden_gradients(pieces, places, grads, shared, slope, value, linear, taps):
    copies = lax.axis_size(Z_ALL)
    peers, padded, width = grads.shape
    z_count, _, share, half = pieces[0].shape
    y_count = 2 * width // share
    rows = width
    saved = pl.BlockSpec((1, padded, half), lambda b, at: (b, 0, 0))
    made = pl.BlockSpec((1, rows, half), lambda b, at: (b, 0, 0))
    small = pl.BlockSpec((3, half), lambda b, at: (0, 0))
    return pl.pallas_call(
        hidden_kernel,
        grid_spec=pltpu.PrefetchScalarGridSpec(
            num_scalar_prefetch=1,
            grid=(2,),
            in_specs=[
                pl.BlockSpec((piece.shape[0], 1, share, half), lambda b, at: (0, 2, 0, 0))
                for piece in pieces
            ]
            + [
                pl.BlockSpec((peers // 2, padded, width), lambda b, at: (b, 0, 0)),
                pl.BlockSpec((peers // 2, padded, width), lambda b, at: (b, 0, 0)),
                saved,
                saved,
                saved,
                small,
            ],
            out_specs=[made, made, pl.BlockSpec((copies, 3, half), lambda b, at: (0, 0, 0))],
            scratch_shapes=[
                pltpu.VMEM((z_count, y_count, share, half), jnp.bfloat16),
                pltpu.VMEM((3, half), jnp.float32),
            ],
        ),
        out_shape=[
            jax.ShapeDtypeStruct((2, rows, half), jnp.bfloat16),
            jax.ShapeDtypeStruct((2, rows, half), jnp.bfloat16),
            jax.ShapeDtypeStruct((copies, 3, half), jnp.float32),
        ],
    )(places, *pieces, grads, shared, slope, value, linear, taps)


def output_kernel(places, *refs):
    pieces, (linear_grad, up_grad, kept, sent, both) = refs[:PIECES], refs[PIECES:]
    _, _, share, half = both.shape
    width = kept.shape[3]
    per_tp = width // share
    z = pl.program_id(0)
    split = pl.num_programs(0) // 2

    def place(at):
        both[:, pl.ds(places[at], 1)] = pieces[at][0][:, None]

    for at in range(PIECES - 2):
        place(at)
    pl.when(z < split)(lambda: place(PIECES - 2))
    pl.when(z >= split)(lambda: place(PIECES - 1))
    contract = (((1,), (1,)), ((), ()))
    core = places[PIECES]
    for target, out in ((core, kept), (1 - core, sent)):
        gate, up = (
            both[part, pl.ds(target * per_tp, per_tp)].reshape(width, half) for part in range(2)
        )
        for b in range(2):
            part = lax.dot_general(
                linear_grad[b], gate, contract, preferred_element_type=jnp.float32
            ) + lax.dot_general(
                up_grad[b], up, contract, preferred_element_type=jnp.float32
            )
            out[b, 0] = part.astype(jnp.bfloat16)


def output_partials(pieces, places, linear_grad, up_grad, width):
    _, rows, half = linear_grad.shape
    z_count, _, share, _ = pieces[0].shape
    mid = pieces[-1].shape[0]
    y_count = 2 * width // share
    whole = pl.BlockSpec((2, rows, half), lambda i, at: (0, 0, 0))
    maps = [lambda i, at: (i, 0, 0, 0)] * (PIECES - 2) + [
        lambda i, at: (jnp.minimum(i, mid - 1), 0, 0, 0),
        lambda i, at: (jnp.maximum(i - mid, 0), 0, 0, 0),
    ]
    made = pl.BlockSpec((2, 1, rows, width), lambda i, at: (0, i, 0, 0))
    shape = jax.ShapeDtypeStruct((2, z_count, rows, width), jnp.bfloat16)
    return pl.pallas_call(
        output_kernel,
        grid_spec=pltpu.PrefetchScalarGridSpec(
            num_scalar_prefetch=1,
            grid=(z_count,),
            in_specs=[pl.BlockSpec((1, 2, share, half), m) for m in maps] + [whole, whole],
            out_specs=[made, made],
            scratch_shapes=[pltpu.VMEM((2, y_count, share, half), jnp.bfloat16)],
        ),
        out_shape=[shape, shape],
    )(places, *pieces, linear_grad, up_grad)


def block_gradients(out_grad, gate_lin, up_lin, conv_weight, gate_weight, up_weight, down_weight):
    rows, columns = gate_lin.shape
    width = out_grad.shape[1]
    half = columns // 2
    second = lax.axis_index("zp") == 1

    own, other = halves_of(jnp.stack([gate_weight, up_weight, down_weight.T]), second)
    pieces, places, late = gathered_y(gathered_z(own, other))

    spare = ((0, 0), (0, columns - width))
    last = jnp.concatenate([gate_lin[-2:], up_lin[-1:], jnp.pad(out_grad[-1:], spare)])
    lead = jnp.concatenate([gate_lin[:2], up_lin[:1], jnp.pad(out_grad[:1], spare)])
    before = to_next(last, SEQ_AXES, 1)
    after = to_next(lead, SEQ_AXES, -1)
    grads = jnp.concatenate(
        [
            before[3:, :width],
            out_grad,
            after[3:, :width],
            jnp.zeros((PAD - rows - 2, width), out_grad.dtype),
        ]
    )
    grads = sent_to_all(grads, ("zp", "x"))
    shared = swapped(grads, "core", 1)

    kept, sent = halves_of(jnp.concatenate([gate_lin, up_lin, before, after]), second)
    came = swapped(sent, "zp", 1)
    kept, came, _ = lax.optimization_barrier((kept, came, late))
    pair = jnp.stack([jnp.where(second, came, kept), jnp.where(second, kept, came)])
    pair = pair.astype(jnp.float32)
    edge = pair[:, 2 * rows :]
    linear = jnp.concatenate([edge[:, :2], pair[:, :rows], edge[:, 4:6]], axis=1)
    up_ext = jnp.concatenate([edge[:, 2:3], pair[:, rows : 2 * rows], edge[:, 6:7]], axis=1)
    start = lax.axis_index(TP) * columns + jnp.where(second, half, 0)
    taps = lax.dynamic_slice_in_dim(conv_weight, start, half, 1).astype(jnp.float32)

    gate = taps[0] * linear[:, :-2] + taps[1] * linear[:, 1:-1] + taps[2] * linear[:, 2:]
    gelu_value, gelu_slope = gelu_parts(gate)

    tail = ((0, 0), (0, PAD - rows - 2), (0, 0))
    linear_grad, up_grad, conv = hidden_gradients(
        pieces,
        places,
        grads,
        shared,
        jnp.pad(up_ext * gelu_slope, tail),
        jnp.pad(gelu_value, tail),
        jnp.pad(linear, ((0, 0), (0, PAD - rows - 4), (0, 0))),
        taps,
    )
    conv = lax.all_to_all(conv, Z_ALL, 0, 0, tiled=True)
    conv = conv.reshape(-1, 2, 3, half).sum(axis=0).transpose(1, 0, 2).reshape(3, columns)
    kept, sent = output_partials(pieces, places, linear_grad, up_grad, width)
    came = swapped(sent, "core", 1)
    product = (kept.astype(jnp.float32) + came.astype(jnp.float32)).astype(jnp.bfloat16)
    conv = sent_to_all(conv, "y")
    conv = conv.sum(axis=0)
    arrived = lax.all_to_all(
        product.reshape(-1, rows, width), ("zp", "x"), 0, 0, tiled=True
    )
    input_grad = arrived.astype(jnp.float32).sum(axis=0).astype(jnp.bfloat16)
    conv = lax.all_gather(conv, TP)
    conv_grad = conv.transpose(1, 0, 2).reshape(3, -1)
    return (input_grad, conv_grad)


def solution(mesh):
    finer = Mesh(
        mesh.devices.reshape(mesh.shape["rep"], 2, 2, 8, 4, 2),
        ("rep", "zk", "zp", "y", "x", "core"),
    )
    return jax.shard_map(
        block_gradients,
        mesh=finer,
        in_specs=(
            P(ROWS, TP),
            P(ROWS, TP),
            P(ROWS, TP),
            P(),
            P(SEQ_AXES, TP),
            P(SEQ_AXES, TP),
            P(TP, SEQ_AXES),
        ),
        out_specs=(P(ROWS, TP), P()),
        check_vma=False,
    )
```

```python
import math

import jax
import jax.numpy as jnp
from jax import lax
from jax.experimental import pallas as pl
from jax.experimental.pallas import tpu as pltpu
from jax.sharding import Mesh
from jax.sharding import PartitionSpec as P


Z_ALL = ("rep", "zk", "zp")
SEQ_AXES = ("zk", "zp", "y")
TP = ("x", "core")
ROWS = ("rep", "zk", "zp", "y")
PAD = 264
PIECES = 9


def shifted(value, axis, by):
    count = lax.axis_size(axis)
    return lax.ppermute(value, axis, [(i, (i + by) % count) for i in range(count)])


def to_next(value, axis, by):
    count = lax.axis_size(axis)
    pairs = [(i, i + by) for i in range(count) if 0 <= i + by < count]
    return lax.ppermute(value, axis, pairs)


def swapped(value, axis, bit):
    return lax.ppermute(value, axis, [(i, i ^ bit) for i in range(lax.axis_size(axis))])


def sent_to_all(value, axis):
    peers = lax.axis_size(axis)
    return lax.all_to_all(
        jnp.broadcast_to(value[None], (peers, *value.shape)), axis, 0, 0, tiled=True
    )


def halves_of(value, second):
    half = value.shape[-1] // 2
    left, right = value[..., :half], value[..., half:]
    return jnp.where(second, right, left), jnp.where(second, left, right)


def crossed(value, axis, by):
    names = axis if isinstance(axis, tuple) else (axis,)
    count = lax.axis_size(names)
    pairs = [
        (2 * i + core, 2 * ((i + step) % count) + core)
        for i in range(count)
        for core, step in enumerate((by, -by))
    ]
    return lax.ppermute(value, (*names, "core"), pairs)


def gathered_z(own, other):
    two_away = crossed(own, Z_ALL, 2)
    above, below = shifted(other, Z_ALL, -1), shifted(other, Z_ALL, 1)
    relative = [own, above, two_away, below]
    count = len(relative)
    at = lax.axis_index(("zk", "zp"))
    return jnp.stack([lax.select_n((place - at) % count, *relative) for place in range(count)])


def gathered_y(block):
    mid = block.shape[0] // 2
    pieces, steps = [block], [0]
    one = two = block
    for k in range(1, 4):
        one, two = shifted(one, "y", 1), shifted(two, "y", -1)
        pieces += [one, two]
        steps += [-k, k]
    pieces += [shifted(one[:mid], "y", 1), shifted(two[mid:], "y", -1)]
    count = lax.axis_size("y")
    places = (lax.axis_index("y") + jnp.array(steps + [4, 4], jnp.int32)) % count
    places = jnp.append(places, lax.axis_index("core"))
    return pieces, places.astype(jnp.int32), pieces[5]


def gelu_parts(gate):
    normal_cdf = 0.5 * (1.0 + jax.scipy.special.erf(gate * (1.0 / math.sqrt(2.0))))
    density = jnp.exp(-0.5 * gate * gate) * (1.0 / math.sqrt(2.0 * math.pi))
    return (gate * normal_cdf, normal_cdf + gate * density)


def hidden_kernel(places, *refs):
    pieces, refs = refs[:PIECES], refs[PIECES:]
    grads, shared, slope, value, linear, taps, linear_out, up_out, conv_out, down, total = refs
    _, padded, width = grads.shape
    rows = linear_out.shape[1]
    z_count, _, share, half = down.shape
    first = pl.program_id(0) == 0

    @pl.when(first)
    def _():
        start = 0
        for at, piece in enumerate(pieces):
            depth = piece.shape[0]
            down[start : start + depth, pl.ds(places[at], 1)] = piece[...]
            start = (start + depth) % z_count

    per_tp = width // share
    act = jnp.zeros(slope.shape[1:], jnp.float32)
    core = places[PIECES]
    for z in range(z_count):
        for part, owner in ((grads, core), (shared, 1 - core)):
            act += jnp.dot(
                part[z],
                down[z, pl.ds(owner * per_tp, per_tp)].reshape(width, half),
                preferred_element_type=jnp.float32,
            )
    grad = act * slope[0]

    def ahead(value, by):
        return pltpu.roll(value, padded - by, 0)

    linear_grad = (
        taps[0:1] * ahead(grad, 2) + taps[1:2] * ahead(grad, 1) + taps[2:3] * grad
    )
    linear_out[0] = linear_grad[:rows].astype(jnp.bfloat16)
    up_out[0] = ahead(act * value[0], 1)[:rows].astype(jnp.bfloat16)
    at = lax.broadcasted_iota(jnp.int32, grad.shape, 0)
    own = jnp.where((at >= 1) & (at <= rows), grad, 0.0)
    near = linear[0].astype(jnp.float32)
    sums = jnp.concatenate(
        [
            jnp.sum(own * (near if k == 0 else ahead(near, k)), axis=0, keepdims=True)
            for k in range(3)
        ]
    )

    @pl.when(first)
    def _():
        total[...] = sums

    @pl.when(jnp.logical_not(first))
    def _():
        conv_out[...] = jnp.broadcast_to((total[...] + sums)[None], conv_out.shape)


def hidden_gradients(pieces, places, grads, shared, slope, value, linear, taps):
    copies = lax.axis_size(Z_ALL)
    peers, padded, width = grads.shape
    z_count, _, share, half = pieces[0].shape
    y_count = 2 * width // share
    rows = width
    saved = pl.BlockSpec((1, padded, half), lambda b, at: (b, 0, 0))
    made = pl.BlockSpec((1, rows, half), lambda b, at: (b, 0, 0))
    small = pl.BlockSpec((3, half), lambda b, at: (0, 0))
    return pl.pallas_call(
        hidden_kernel,
        grid_spec=pltpu.PrefetchScalarGridSpec(
            num_scalar_prefetch=1,
            grid=(2,),
            in_specs=[
                pl.BlockSpec((piece.shape[0], 1, share, half), lambda b, at: (0, 2, 0, 0))
                for piece in pieces
            ]
            + [
                pl.BlockSpec((peers // 2, padded, width), lambda b, at: (b, 0, 0)),
                pl.BlockSpec((peers // 2, padded, width), lambda b, at: (b, 0, 0)),
                saved,
                saved,
                saved,
                small,
            ],
            out_specs=[made, made, pl.BlockSpec((copies, 3, half), lambda b, at: (0, 0, 0))],
            scratch_shapes=[
                pltpu.VMEM((z_count, y_count, share, half), jnp.bfloat16),
                pltpu.VMEM((3, half), jnp.float32),
            ],
        ),
        out_shape=[
            jax.ShapeDtypeStruct((2, rows, half), jnp.bfloat16),
            jax.ShapeDtypeStruct((2, rows, half), jnp.bfloat16),
            jax.ShapeDtypeStruct((copies, 3, half), jnp.float32),
        ],
    )(places, *pieces, grads, shared, slope, value, linear, taps)


def output_kernel(places, *refs):
    pieces, (linear_grad, up_grad, kept, sent, both) = refs[:PIECES], refs[PIECES:]
    _, _, share, half = both.shape
    width = kept.shape[3]
    per_tp = width // share
    z = pl.program_id(0)
    split = pl.num_programs(0) // 2

    def place(at):
        both[:, pl.ds(places[at], 1)] = pieces[at][0][:, None]

    for at in range(PIECES - 2):
        place(at)
    pl.when(z < split)(lambda: place(PIECES - 2))
    pl.when(z >= split)(lambda: place(PIECES - 1))
    contract = (((1,), (1,)), ((), ()))
    core = places[PIECES]
    for target, out in ((core, kept), (1 - core, sent)):
        gate, up = (
            both[part, pl.ds(target * per_tp, per_tp)].reshape(width, half) for part in range(2)
        )
        for b in range(2):
            part = lax.dot_general(
                linear_grad[b], gate, contract, preferred_element_type=jnp.float32
            ) + lax.dot_general(
                up_grad[b], up, contract, preferred_element_type=jnp.float32
            )
            out[b, 0] = part.astype(jnp.bfloat16)


def output_partials(pieces, places, linear_grad, up_grad, width):
    _, rows, half = linear_grad.shape
    z_count, _, share, _ = pieces[0].shape
    mid = pieces[-1].shape[0]
    y_count = 2 * width // share
    whole = pl.BlockSpec((2, rows, half), lambda i, at: (0, 0, 0))
    maps = [lambda i, at: (i, 0, 0, 0)] * (PIECES - 2) + [
        lambda i, at: (jnp.minimum(i, mid - 1), 0, 0, 0),
        lambda i, at: (jnp.maximum(i - mid, 0), 0, 0, 0),
    ]
    made = pl.BlockSpec((2, 1, rows, width), lambda i, at: (0, i, 0, 0))
    shape = jax.ShapeDtypeStruct((2, z_count, rows, width), jnp.bfloat16)
    return pl.pallas_call(
        output_kernel,
        grid_spec=pltpu.PrefetchScalarGridSpec(
            num_scalar_prefetch=1,
            grid=(z_count,),
            in_specs=[pl.BlockSpec((1, 2, share, half), m) for m in maps] + [whole, whole],
            out_specs=[made, made],
            scratch_shapes=[pltpu.VMEM((2, y_count, share, half), jnp.bfloat16)],
        ),
        out_shape=[shape, shape],
    )(places, *pieces, linear_grad, up_grad)


def block_gradients(out_grad, gate_lin, up_lin, conv_weight, gate_weight, up_weight, down_weight):
    rows, columns = gate_lin.shape
    width = out_grad.shape[1]
    half = columns // 2
    second = lax.axis_index("zp") == 1

    own, other = halves_of(jnp.stack([gate_weight, up_weight, down_weight.T]), second)
    pieces, places, late = gathered_y(gathered_z(own, other))

    spare = ((0, 0), (0, columns - width))
    last = jnp.concatenate([gate_lin[-2:], up_lin[-1:], jnp.pad(out_grad[-1:], spare)])
    lead = jnp.concatenate([gate_lin[:2], up_lin[:1], jnp.pad(out_grad[:1], spare)])
    before = to_next(last, SEQ_AXES, 1)
    after = to_next(lead, SEQ_AXES, -1)
    grads = jnp.concatenate(
        [
            before[3:, :width],
            out_grad,
            after[3:, :width],
            jnp.zeros((PAD - rows - 2, width), out_grad.dtype),
        ]
    )
    grads = sent_to_all(grads, ("zp", "x"))
    shared = swapped(grads, "core", 1)

    kept, sent = halves_of(jnp.concatenate([gate_lin, up_lin, before, after]), second)
    came = swapped(sent, "zp", 1)
    kept, came, _ = lax.optimization_barrier((kept, came, late))
    pair = jnp.stack([jnp.where(second, came, kept), jnp.where(second, kept, came)])
    pair = pair.astype(jnp.float32)
    edge = pair[:, 2 * rows :]
    linear = jnp.concatenate([edge[:, :2], pair[:, :rows], edge[:, 4:6]], axis=1)
    up_ext = jnp.concatenate([edge[:, 2:3], pair[:, rows : 2 * rows], edge[:, 6:7]], axis=1)
    start = lax.axis_index(TP) * columns + jnp.where(second, half, 0)
    taps = lax.dynamic_slice_in_dim(conv_weight, start, half, 1).astype(jnp.float32)
    gate = taps[0] * linear[:, :-2] + taps[1] * linear[:, 1:-1] + taps[2] * linear[:, 2:]
    gelu_value, gelu_slope = gelu_parts(gate)

    tail = ((0, 0), (0, PAD - rows - 2), (0, 0))
    linear_grad, up_grad, conv = hidden_gradients(
        pieces,
        places,
        grads,
        shared,
        jnp.pad(up_ext * gelu_slope, tail),
        jnp.pad(gelu_value, tail),
        jnp.pad(linear, ((0, 0), (0, PAD - rows - 4), (0, 0))).astype(jnp.bfloat16),
        taps,
    )
    conv = lax.all_to_all(conv, Z_ALL, 0, 0, tiled=True)
    conv = conv.reshape(-1, 2, 3, half).sum(axis=0).transpose(1, 0, 2).reshape(3, columns)
    kept, sent = output_partials(pieces, places, linear_grad, up_grad, width)
    came = swapped(sent, "core", 1)
    product = (kept.astype(jnp.float32) + came.astype(jnp.float32)).astype(jnp.bfloat16)
    conv = sent_to_all(conv, "y")
    conv = conv.sum(axis=0)
    arrived = lax.all_to_all(
        product.reshape(-1, rows, width), ("zp", "x"), 0, 0, tiled=True
    )
    input_grad = arrived.astype(jnp.float32).sum(axis=0).astype(jnp.bfloat16)
    conv = lax.all_gather(conv, TP)
    conv_grad = conv.transpose(1, 0, 2).reshape(3, -1)
    return (input_grad, conv_grad)


def solution(mesh):
    finer = Mesh(
        mesh.devices.reshape(mesh.shape["rep"], 2, 2, 8, 4, 2),
        ("rep", "zk", "zp", "y", "x", "core"),
    )
    return jax.shard_map(
        block_gradients,
        mesh=finer,
        in_specs=(
            P(ROWS, TP),
            P(ROWS, TP),
            P(ROWS, TP),
            P(),
            P(SEQ_AXES, TP),
            P(SEQ_AXES, TP),
            P(TP, SEQ_AXES),
        ),
        out_specs=(P(ROWS, TP), P()),
        check_vma=False,
    )
```
